512 devices in a mesh: grp: 2 (over y), ep: 64 (over z, core), tp: 4 (over x).
Axes of the slice: x: 4, y: 2, z: 32, core: 2. Of those that a mesh axis runs over, the one named last changes fastest.
The devices are a block of a 4x8x32 slice.
Arguments:
- tokens: bfloat16 [49152, 2048], P(('grp', 'ep'), 'tp'), parts along dimension 0
- group_choice: int32 [49152], P(('grp', 'ep')), parts along dimension 0, may hold values from 0 to 7, as said below
- expert_choice: int32 [49152, 2], P(('grp', 'ep')), parts along dimension 0, may hold values from 0 to 7, as said below
- group_weight: float32 [49152], P(('grp', 'ep')), parts along dimension 0, may hold values from 0.3 to 1
- expert_weight: float32 [49152, 2], P(('grp', 'ep')), parts along dimension 0, may hold values from 0.1 to 1
- norm_gain: float32 [2048], replicated, may hold values from 0.1 to 1.9
- w_gate: bfloat16 [64, 2048, 1024], P('ep', None, 'tp'), may hold values from -0.125 to 0.125
- w_up: bfloat16 [64, 2048, 1024], P('ep', None, 'tp'), may hold values from -0.125 to 0.125
- w_down: bfloat16 [64, 1024, 2048], P('ep', None, 'tp'), may hold values from -0.1875 to 0.1875
Outputs:
- moe_out: bfloat16 [49152, 2048], P(('grp', 'ep'), 'tp'), parts along dimension 0
The draws below stay inside these ranges and needn't reach their ends.
There are 2 independent parts, one for each index of `grp`. The reference program is written for one: setup_inputs(seed, part) draws one part's arguments, and reference() takes and returns one part's arrays. A program takes and returns all parts, laid end to end along the dimension named above; an argument that names none is the same for every part. Nothing has to cross between parts.
Inputs may be any that keep to these rules, and one draw needn't show every extreme that they name: `group_choice`: group of each token, 0 to 7; within each aligned block of 384 tokens (the tokens of one index of ep) every group is chosen by the same number of tokens. `expert_choice`: a token's two entries differ; within each aligned block of 384 tokens no expert (group with entry) is named by more than 18 tokens, and in every block one expert of each group, the same one in all blocks, is named by exactly 18 tokens.
All inputs are finite; a program needn't handle non-finite values.
Results may differ from the reference program's by a relative error of at most 0.0071.
Values may be sent and summed in bfloat16 or wider, within the bound.
No kernel may reach another device: no remote copies, remote signals or barrier semaphores. Data moves between devices by JAX's collectives and lax.ppermute only.
A program may use at most 64 MiB of HBM per device.

```python
import math
import jax
import jax.numpy as jnp
from jax import lax

D = 2048
FF = 1024
TOK_DEV = 384
TOP_K = 2
EXPERTS = 64
EXPERTS_GROUP = 8
GROUPS = 8
CAP = 18
TOKENS = 24576


def route_tables(key):
    base = jax.random.fold_in(key, 11)
    per_group = TOK_DEV // GROUPS
    mean_load = 2 * per_group // EXPERTS_GROUP
    swing = min(mean_load // 2, per_group - mean_load)
    pairs = EXPERTS_GROUP // 2
    blocks = TOKENS // TOK_DEV
    order_keys = jax.random.split(jax.random.fold_in(base, 1), GROUPS)
    orders = jax.vmap(lambda one_key: jax.random.permutation(one_key, EXPERTS_GROUP))(order_keys)

    def one_block(block_key):
        key_shift, key_seat, key_flip = jax.random.split(block_key, 3)
        shifts = jax.random.randint(key_shift, (GROUPS, pairs), -swing, swing + 1)
        shifts = shifts.at[:, 0].set(swing)
        loads = jnp.stack([mean_load + shifts, mean_load - shifts], -1).reshape(GROUPS, EXPERTS_GROUP)
        placed = jnp.zeros((GROUPS, EXPERTS_GROUP), jnp.int32).at[jnp.arange(GROUPS)[:, None], orders].set(loads.astype(jnp.int32))
        ends = jnp.cumsum(placed, -1)
        spots = jnp.arange(2 * per_group, dtype=jnp.int32)
        labels = jnp.sum((spots[None, :, None] >= ends[:, None, :]).astype(jnp.int32), -1)
        first = labels[:, :per_group].reshape(-1)
        second = labels[:, per_group:].reshape(-1)
        flips = jax.random.randint(key_flip, (TOK_DEV,), 0, 2)
        first_swapped = jnp.where(flips == 1, second, first)
        second_swapped = jnp.where(flips == 1, first, second)
        seats = jax.random.permutation(key_seat, TOK_DEV)
        group_rank = (jnp.arange(TOK_DEV, dtype=jnp.int32) // per_group).astype(jnp.int32)
        group_of = jnp.zeros((TOK_DEV,), jnp.int32).at[seats].set(group_rank)
        first_of = jnp.zeros((TOK_DEV,), jnp.int32).at[seats].set(first_swapped)
        second_of = jnp.zeros((TOK_DEV,), jnp.int32).at[seats].set(second_swapped)
        return (group_of, jnp.stack([first_of, second_of], -1))
    block_keys = jax.random.split(jax.random.fold_in(base, 2), blocks)
    groups_all, experts_all = jax.vmap(one_block)(block_keys)
    return (groups_all.reshape(TOKENS), experts_all.reshape(TOKENS, TOP_K))


def draw_group_choice(key, part):
    return route_tables(key)[0]


def draw_expert_choice(key, part):
    return route_tables(key)[1]


def draw_tokens(key, part):
    key_main = jax.random.fold_in(jax.random.fold_in(key, 5), 0)
    column_scale = jnp.exp(math.log(4.0) * jnp.arange(D, dtype=jnp.float32) / D)
    values = jax.random.normal(key_main, (TOKENS, D), jnp.float32)
    return (values * column_scale[None, :]).astype(jnp.bfloat16)


def shard_levels(rng, shape, pieces, low, top_value):
    gain = 1.0
    for axis_at, parts in pieces:
        steps = jax.random.uniform(jax.random.fold_in(jax.random.fold_in(rng, 6), axis_at), (parts,), jnp.float32, low / len(pieces), top_value / len(pieces))
        gain = gain * jnp.repeat(jnp.exp(steps), shape[axis_at] // parts).reshape((-1,) + (1,) * (len(shape) - 1 - axis_at))
    return gain


def bell_draw(own_key, shape, deviation, most, cuts=(), held_as=jnp.bfloat16):
    values = deviation * jax.random.normal(own_key, shape, jnp.float32)
    if cuts:
        values = values * shard_levels(own_key, shape, cuts, -0.22, 0.18)
    return jnp.clip(values, -most, most).astype(held_as)


def setup_inputs(seed: int = 0, part: int = 0) -> dict:
    key_list = jax.random.split(jax.random.key(seed), 10)
    part_splits = jax.random.split(jax.random.fold_in(key_list[9], part), 10)
    return {
        "tokens": draw_tokens(jax.random.fold_in(jax.random.fold_in(key_list[9], part), 71), part),
        "group_choice": draw_group_choice(jax.random.fold_in(jax.random.fold_in(key_list[9], part), 71), part),
        "expert_choice": draw_expert_choice(jax.random.fold_in(jax.random.fold_in(key_list[9], part), 71), part),
        "group_weight": jnp.clip(0.3 + 0.7 * jax.random.uniform(part_splits[3], (TOKENS,), jnp.float32) ** shard_levels(part_splits[3], (TOKENS,), ((0, 64),), -0.2, 0.2), 0.3, 1.0),
        "expert_weight": jnp.clip(jnp.exp(math.log(1.0) - 2.3025851 * jax.random.uniform(part_splits[4], (TOKENS, TOP_K), jnp.float32) ** shard_levels(part_splits[4], (TOKENS, TOP_K), ((0, 64),), -0.2, 0.2)), 0.1, 1.0),
        "norm_gain": jnp.clip(1.0 + 0.18 * jax.random.normal(key_list[5], (D,), jnp.float32), 0.1, 1.9),
        "w_gate": bell_draw(key_list[6], (EXPERTS, D, FF), D ** -0.5, 0.125, ((0, 64), (2, 4))),
        "w_up": bell_draw(key_list[7], (EXPERTS, D, FF), D ** -0.5, 0.125, ((0, 64), (2, 4))),
        "w_down": bell_draw(key_list[8], (EXPERTS, FF, D), FF ** -0.5, 0.1875, ((0, 64), (2, 4))),
    }


def reference(tokens, group_choice, expert_choice, group_weight, expert_weight, norm_gain, w_gate, w_up, w_down):
    values = tokens.astype(jnp.float32)
    inv_rms = lax.rsqrt(lax.optimization_barrier(jnp.mean(values * values, -1, keepdims=True)) + 1e-06)
    normed = (values * inv_rms * norm_gain.astype(jnp.float32)).astype(jnp.bfloat16)
    expert_ids = (group_choice[:, None] * EXPERTS_GROUP + expert_choice).astype(jnp.int32)
    mixing = group_weight[:, None] * expert_weight / lax.optimization_barrier(jnp.sum(expert_weight, -1, keepdims=True))
    flat_ids = expert_ids.reshape(-1)
    flat_tokens = jnp.repeat(jnp.arange(TOKENS, dtype=jnp.int32), TOP_K)
    flat_mix = mixing.reshape(-1)
    ordering = jnp.argsort(flat_ids, stable=True).astype(jnp.int32)
    sorted_tokens = flat_tokens[ordering]
    sorted_mix = flat_mix[ordering]
    counts = lax.optimization_barrier(jnp.sum((flat_ids[None, :] == jnp.arange(EXPERTS, dtype=jnp.int32)[:, None]).astype(jnp.int32), 1))
    starts = jnp.cumsum(counts) - counts
    rows_most = TOKENS // TOK_DEV * CAP
    offsets = jnp.arange(rows_most, dtype=jnp.int32)

    def per_expert(summed, expert):
        places = jnp.minimum(starts[expert] + offsets, TOKENS * TOP_K - 1).astype(jnp.int32)
        alive = offsets < counts[expert]
        token_rows = sorted_tokens[places]
        weights = jnp.where(alive, sorted_mix[places], 0.0)
        chosen = normed[token_rows]
        gate_sum = jnp.dot(chosen, w_gate[expert], preferred_element_type=jnp.float32)
        up_sum = jnp.dot(chosen, w_up[expert], preferred_element_type=jnp.float32)
        hidden = (jax.nn.silu(gate_sum) * up_sum).astype(jnp.bfloat16)
        result = jnp.dot(hidden, w_down[expert], preferred_element_type=jnp.float32).astype(jnp.bfloat16)
        summed = summed.at[token_rows].add(result.astype(jnp.float32) * weights[:, None])
        return (summed, None)
    initial = jnp.zeros((TOKENS, D), jnp.float32)
    summed, _ = lax.scan(per_expert, initial, jnp.arange(EXPERTS, dtype=jnp.int32))
    return summed.astype(jnp.bfloat16)
```

```python
import jax
import jax.numpy as jnp
from jax import lax
from jax.sharding import Mesh
from jax.sharding import PartitionSpec as P

GROUP_SIZE = 8
EP = ("g", "m")
GRP_EP = ("grp", "g", "m")


def exchange(array, axis):
    return lax.all_to_all(array, axis, 0, 0, tiled=True)


def shifted(array, axis, by):
    length = lax.axis_size(axis)
    return lax.ppermute(array, axis, [(a, (a + by) % length) for a in range(length)])


def ring_pieces(array, axis):
    half = array.shape[0] // 2
    one = shifted(array, axis, 1)
    three = shifted(array, axis, 3)
    top = shifted(one[:half], axis, 1)
    bottom = shifted(three[half:], axis, 3)
    return [array, one, three, jnp.concatenate([top, bottom], 0)], (0, 3, 1, 2)


def ring_dot(pieces, offsets, weights, axis):
    me = lax.axis_index(axis)
    depth = weights[0].shape[0] // lax.axis_size(axis)
    sums = [None] * len(weights)
    for piece, offset in zip(pieces, offsets, strict=True):
        owner = lax.rem(me + offset, lax.axis_size(axis))
        for i, weight in enumerate(weights):
            part = lax.dynamic_slice_in_dim(weight, owner * depth, depth, 0)
            product = jnp.dot(piece, part, preferred_element_type=jnp.float32)
            sums[i] = product if sums[i] is None else sums[i] + product
    return sums


def body(
    tokens,
    group_choice,
    expert_choice,
    group_weight,
    expert_weight,
    norm_gain,
    w_gate,
    w_up,
    w_down,
):
    tok_rows, piece_width = tokens.shape
    groups = lax.axis_size("g")
    members = lax.axis_size("m")
    per_group = tok_rows // groups
    mean_load = 2 * tok_rows // (groups * members)
    capacity = mean_load + min(mean_load // 2, per_group - mean_load)
    model_width = norm_gain.shape[0]
    tp_count = lax.axis_size("tp")

    values = tokens.astype(jnp.float32)
    own_squares = jnp.sum(values * values, -1)
    all_squares = jnp.sum(
        exchange(jnp.broadcast_to(own_squares[None, None], (tp_count, 1, tok_rows)), "tp"), (0, 1)
    )
    inv_rms = lax.rsqrt(all_squares / model_width + 1e-06)
    gain_piece = lax.dynamic_slice_in_dim(
        norm_gain, lax.axis_index("tp") * piece_width, piece_width, 0
    )

    in_group = group_choice[:, None] == jnp.arange(groups, dtype=jnp.int32)[None, :]
    before = jnp.tril(jnp.ones((tok_rows, tok_rows), jnp.bfloat16), -1)
    ranks = jnp.dot(before, in_group.astype(jnp.bfloat16), preferred_element_type=jnp.float32)
    rank = jnp.sum(jnp.where(in_group, ranks, 0.0), 1).astype(jnp.int32)
    slot = group_choice * per_group + rank
    slots = jnp.arange(tok_rows, dtype=jnp.int32)
    seating = slots[:, None] == slot[None, :]

    mixing = group_weight[:, None] * expert_weight / jnp.sum(expert_weight, -1, keepdims=True)
    facts = [expert_choice[:, 0].astype(jnp.float32), expert_choice[:, 1].astype(jnp.float32)]
    facts += [mixing[:, 0], mixing[:, 1]]
    facts = jnp.stack([jnp.sum(jnp.where(seating, f[None, :], 0.0), 1) for f in facts])
    facts = exchange(facts.reshape(4, groups, per_group).swapaxes(0, 1), "g")
    facts = facts.swapaxes(0, 1).reshape(4, tok_rows)
    choices = facts[:2].astype(jnp.int32)
    shares = facts[2:]

    normed = (values * inv_rms[:, None] * gain_piece[None, :]).astype(jnp.bfloat16)
    seated = jnp.dot(
        seating.astype(jnp.bfloat16), normed, preferred_element_type=jnp.float32
    ).astype(jnp.bfloat16)
    landed = exchange(seated.reshape(groups, per_group, piece_width), "g")
    landed = landed.reshape(tok_rows, piece_width)

    experts = jnp.arange(members, dtype=jnp.int32)
    named = (choices[0][:, None] == experts) | (choices[1][:, None] == experts)
    block = slots // per_group
    same_block = (block[:, None] == block[None, :]) & (slots[:, None] > slots[None, :])
    earlier = jnp.dot(
        same_block.astype(jnp.bfloat16),
        named.astype(jnp.bfloat16),
        preferred_element_type=jnp.float32,
    )
    seats = groups * capacity
    places = jnp.arange(members * seats, dtype=jnp.int32)
    targets = []
    for k in range(2):
        chosen = choices[k][:, None] == experts
        seat = jnp.sum(jnp.where(chosen, earlier, 0.0), 1).astype(jnp.int32)
        targets.append(choices[k] * seats + block * capacity + seat)
    spread = (places[:, None] == targets[0][None, :]) | (places[:, None] == targets[1][None, :])
    buffer = jnp.dot(
        spread.astype(jnp.bfloat16), landed, preferred_element_type=jnp.float32
    ).astype(jnp.bfloat16)
    rows = exchange(buffer.reshape(members, seats, piece_width), "m")
    rows = rows.reshape(members * seats, piece_width)

    pieces, offsets = ring_pieces(rows, "tp")
    gate, up = ring_dot(pieces, offsets, [w_gate[0], w_up[0]], "tp")
    hidden = (jax.nn.silu(gate) * up).astype(jnp.bfloat16)
    pieces, offsets = ring_pieces(hidden, "tp")
    (summed,) = ring_dot(pieces, offsets, [w_down[0]], "tp")
    results = summed.astype(jnp.bfloat16).reshape(members, seats, piece_width)

    returned = exchange(results, "m").reshape(members * seats, piece_width)
    combined = jnp.zeros((tok_rows, piece_width), jnp.float32)
    for k in range(2):
        picker = (targets[k][:, None] == places[None, :]).astype(jnp.bfloat16)
        picked = jnp.dot(picker, returned, preferred_element_type=jnp.float32)
        combined = combined + shares[k][:, None] * picked
    home = exchange(
        combined.astype(jnp.bfloat16).reshape(groups, per_group, piece_width), "g"
    ).reshape(tok_rows, piece_width)
    unseating = slot[:, None] == slots[None, :]
    return jnp.dot(
        unseating.astype(jnp.bfloat16), home, preferred_element_type=jnp.float32
    ).astype(jnp.bfloat16)


def solution(mesh):
    groups = mesh.shape["ep"] // GROUP_SIZE
    split = Mesh(
        mesh.devices.reshape(mesh.shape["grp"], groups, GROUP_SIZE, mesh.shape["tp"]),
        ("grp", "g", "m", "tp"),
    )
    placed = (
        P(GRP_EP, "tp"),
        P(GRP_EP),
        P(GRP_EP, None),
        P(GRP_EP),
        P(GRP_EP, None),
        P(),
        P(EP, None, "tp"),
        P(EP, None, "tp"),
        P(EP, None, "tp"),
    )
    return jax.shard_map(
        body, mesh=split, in_specs=placed, out_specs=P(GRP_EP, "tp"), check_vma=False
    )
```

```python
import jax
import jax.numpy as jnp
from jax import lax
from jax.sharding import Mesh
from jax.sharding import PartitionSpec as P


GROUP_SIZE = 8
TILE = 8
EP = ("g", "m")
GRP_EP = ("grp", "g", "m")
BLOCK = ("tp", "m")


def exchange(array, axis):
    return lax.all_to_all(array, axis, 0, 0, tiled=True)


def shifted(array, axis, by):
    length = lax.axis_size(axis)
    return lax.ppermute(array, axis, [(a, (a + by) % length) for a in range(length)])


def up_to(length, tile):
    return -(-length // tile) * tile


def around(array, axis):
    one = shifted(array, axis, 3)
    three = shifted(array, axis, 1)
    half = array.shape[0] // 2
    top = shifted(one[:half], axis, 3)
    bottom = shifted(three[half:], axis, 1)
    return [(array,), (one,), (top, bottom), (three,)]


def dot(a, b):
    return jnp.dot(a, b, preferred_element_type=jnp.float32)


def dot_parts(a, parts):
    total, at = None, 0
    for part in parts:
        product = dot(a[:, at : at + part.shape[0]], part)
        total = product if total is None else total + product
        at += part.shape[0]
    return total


def layer(
    tokens,
    group_choice,
    expert_choice,
    group_weight,
    expert_weight,
    norm_gain,
    w_gate,
    w_up,
    w_down,
):
    tok_rows, piece_width = tokens.shape
    groups = lax.axis_size("g")
    members = lax.axis_size("m")
    tp_count = lax.axis_size("tp")
    me = lax.axis_index("tp")
    per_group = tok_rows // groups
    mean_load = 2 * tok_rows // (groups * members)
    capacity = mean_load + min(mean_load // 2, per_group - mean_load)
    model_width = norm_gain.shape[0]
    units = w_gate.shape[2]
    width = per_group + TILE

    fused = jnp.concatenate([w_gate[0], w_up[0]], 1)
    ring_in = around(fused, "tp")
    ring_out = around(w_down[0], "tp")

    values = tokens.astype(jnp.float32)
    own_squares = jnp.sum(values * values, -1)
    all_squares = exchange(jnp.broadcast_to(own_squares[None, None], (tp_count, 1, tok_rows)), "tp")
    all_squares = jnp.sum(all_squares, (0, 1))
    inv_rms = lax.rsqrt(all_squares / model_width + 1e-06)
    gain_piece = lax.dynamic_slice_in_dim(norm_gain, me * piece_width, piece_width, 0)

    in_group = group_choice[:, None] == jnp.arange(groups, dtype=jnp.int32)[None, :]
    before = jnp.tril(jnp.ones((tok_rows, tok_rows), jnp.bfloat16), -1)
    ranks = dot(before, in_group.astype(jnp.bfloat16))
    rank = jnp.sum(jnp.where(in_group, ranks, 0.0), 1).astype(jnp.int32)

    mixing = group_weight[:, None] * expert_weight / jnp.sum(expert_weight, -1, keepdims=True)
    coarse = lax.reduce_precision(mixing, 8, 7)
    facts = [expert_choice[:, 0].astype(jnp.float32), expert_choice[:, 1].astype(jnp.float32)]
    facts += [coarse[:, 0], coarse[:, 1]]
    facts += [mixing[:, 0] - coarse[:, 0], mixing[:, 1] - coarse[:, 1]]
    lines = jnp.arange(groups * width, dtype=jnp.int32)
    line_fact = (lines % width - per_group)[:, None]
    spoken = jnp.zeros((groups * width, tok_rows), jnp.float32)
    for i, fact in enumerate(facts):
        spoken = jnp.where(line_fact == i, fact[None, :], spoken)
    spoken = jnp.where((lines // width)[:, None] == group_choice[None, :], spoken, 0.0)
    columns = rank[:, None] == jnp.arange(piece_width, dtype=jnp.int32)[None, :]
    told = dot(spoken.astype(jnp.bfloat16), columns.astype(jnp.bfloat16)).astype(jnp.bfloat16)

    normed = (values * inv_rms[:, None] * gain_piece[None, :]).astype(jnp.bfloat16)
    seating = lines[:, None] == (group_choice * width + rank)[None, :]
    seated = (dot(seating.astype(jnp.bfloat16), normed) + told.astype(jnp.float32)).astype(
        jnp.bfloat16
    )
    landed = exchange(seated.reshape(groups, width, piece_width), "g")

    heard = landed[:, per_group:, :width].astype(jnp.float32)
    choices = [heard[:, k].astype(jnp.int32) for k in range(2)]
    shares = [heard[:, 2 + k] + heard[:, 4 + k] for k in range(2)]
    experts = jnp.arange(members, dtype=jnp.int32)[None, :, None]
    inside = jnp.arange(width, dtype=jnp.int32)[None, :] < per_group
    chosen = [(choices[k][:, None, :] == experts) & inside[:, None, :] for k in range(2)]
    named = (chosen[0] | chosen[1]).astype(jnp.bfloat16).reshape(groups * members, width)
    after = jnp.triu(jnp.ones((width, width), jnp.bfloat16), 1)
    earlier = dot(named, after).reshape(groups, members, width)
    sources = groups // tp_count
    slots = sources * capacity
    depth = up_to(slots, TILE)
    block = jnp.arange(groups, dtype=jnp.int32)[:, None]
    targets = []
    for k in range(2):
        seat = jnp.sum(jnp.where(chosen[k], earlier, 0.0), 1).astype(jnp.int32)
        place = (block // sources * members + choices[k]) * depth
        place = place + block % sources * capacity + seat
        targets.append(jnp.where(inside, place, -1))
    places = jnp.arange(tp_count * members * depth, dtype=jnp.int32)
    flat = [t.reshape(-1) for t in targets]
    spread = (places[:, None] == flat[0][None, :]) | (places[:, None] == flat[1][None, :])
    buffer = dot(
        spread.astype(jnp.bfloat16), landed.reshape(groups * width, piece_width)
    ).astype(jnp.bfloat16)

    rows = exchange(buffer.reshape(tp_count * members, depth, piece_width), BLOCK)
    rows = rows.reshape(tp_count, members * depth, piece_width)
    rows = jnp.concatenate([rows[t] for t in range(tp_count)], 1)
    hidden = []
    for parts in ring_in:
        both = dot_parts(rows, parts)
        hidden.append((jax.nn.silu(both[:, :units]) * both[:, units:]).astype(jnp.bfloat16))
    start = lax.rem(tp_count - me, tp_count)
    hidden = lax.dynamic_slice_in_dim(
        jnp.concatenate(hidden + hidden[:-1], 1), start * units, tp_count * units, 1
    )
    results = [dot_parts(hidden, parts).astype(jnp.bfloat16) for parts in ring_out]
    results = lax.dynamic_slice_in_dim(jnp.stack(results + results[:-1]), start, tp_count, 0)

    returned = exchange(results.reshape(tp_count * members, depth, piece_width), BLOCK)
    returned = returned.reshape(-1, piece_width)
    combined = jnp.zeros((tok_rows, piece_width), jnp.float32)
    for k in range(2):
        back = targets[k][:, :per_group].reshape(-1)
        share = shares[k][:, :per_group].reshape(-1)
        picker = (back[:, None] == places[None, :]).astype(jnp.bfloat16)
        combined = combined + share[:, None] * dot(picker, returned)
    combined = combined.astype(jnp.bfloat16)
    home = exchange(combined.reshape(groups, per_group, piece_width), "g")
    home = home.reshape(tok_rows, piece_width)
    here = lax.axis_index("g")
    seats = jnp.arange(per_group, dtype=jnp.int32)[None, :]
    stayed = (group_choice == here)[:, None] & (rank[:, None] == seats)
    own = lax.dynamic_slice_in_dim(combined, here * per_group, per_group, 0)
    kept = dot(stayed.astype(jnp.bfloat16), own)
    slot = jnp.where(group_choice == here, -1, group_choice * per_group + rank)
    unseating = slot[:, None] == jnp.arange(tok_rows, dtype=jnp.int32)[None, :]
    return (dot(unseating.astype(jnp.bfloat16), home) + kept).astype(jnp.bfloat16)


def solution(mesh):
    groups = mesh.shape["ep"] // GROUP_SIZE
    split = Mesh(
        mesh.devices.reshape(mesh.shape["grp"], groups, GROUP_SIZE, mesh.shape["tp"]),
        ("grp", "g", "m", "tp"),
    )
    placed = (
        P(GRP_EP, "tp"),
        P(GRP_EP),
        P(GRP_EP, None),
        P(GRP_EP),
        P(GRP_EP, None),
        P(),
        P(EP, None, "tp"),
        P(EP, None, "tp"),
        P(EP, None, "tp"),
    )
    return jax.shard_map(
        layer, mesh=split, in_specs=placed, out_specs=P(GRP_EP, "tp"), check_vma=False
    )
```

```python
import jax
import jax.numpy as jnp
from jax import lax
from jax.sharding import Mesh
from jax.sharding import PartitionSpec as P


GROUP_SIZE = 8
TILE = 8
EP = ("g", "m")
GRP_EP = ("grp", "g", "m")
BLOCK = ("tp", "m")


def exchange(array, axis):
    return lax.all_to_all(array, axis, 0, 0, tiled=True)


def shifted(array, axis, by):
    length = lax.axis_size(axis)
    return lax.ppermute(array, axis, [(a, (a + by) % length) for a in range(length)])


def up_to(length, tile):
    return -(-length // tile) * tile


def around(array, axis):
    one = shifted(array, axis, 3)
    three = shifted(array, axis, 1)
    half = array.shape[0] // 2
    top = shifted(one[:half], axis, 3)
    bottom = shifted(three[half:], axis, 1)
    return [(array,), (one,), (top, bottom), (three,)]


def dot(a, b):
    return jnp.dot(a, b, preferred_element_type=jnp.float32)


def dot_parts(a, parts):
    total, at = None, 0
    for part in parts:
        product = dot(a[:, at : at + part.shape[0]], part)
        total = product if total is None else total + product
        at += part.shape[0]
    return total


def layer(
    tokens,
    group_choice,
    expert_choice,
    group_weight,
    expert_weight,
    norm_gain,
    w_gate,
    w_up,
    w_down,
):
    tok_rows, piece_width = tokens.shape
    groups = lax.axis_size("g")
    members = lax.axis_size("m")
    tp_count = lax.axis_size("tp")
    me = lax.axis_index("tp")
    per_group = tok_rows // groups
    mean_load = 2 * tok_rows // (groups * members)
    capacity = mean_load + min(mean_load // 2, per_group - mean_load)
    model_width = norm_gain.shape[0]
    units = w_gate.shape[2]
    width = per_group + TILE

    ring_out = around(w_down[0], "tp")
    ring_in = around(jnp.concatenate([w_gate[0], w_up[0]], 1), "tp")

    in_group = group_choice[:, None] == jnp.arange(groups, dtype=jnp.int32)[None, :]
    before = jnp.tril(jnp.ones((tok_rows, tok_rows), jnp.bfloat16), -1)
    ranks = dot(before, in_group.astype(jnp.bfloat16))
    rank = jnp.sum(jnp.where(in_group, ranks, 0.0), 1).astype(jnp.int32)

    mixing = group_weight[:, None] * expert_weight / jnp.sum(expert_weight, -1, keepdims=True)
    coarse = lax.reduce_precision(mixing, 8, 7)
    facts = [expert_choice[:, 0].astype(jnp.float32), expert_choice[:, 1].astype(jnp.float32)]
    facts += [coarse[:, 0], coarse[:, 1]]
    facts += [mixing[:, 0] - coarse[:, 0], mixing[:, 1] - coarse[:, 1]]
    lines = jnp.arange(groups * width, dtype=jnp.int32)
    line_fact = (lines % width - per_group)[:, None]
    spoken = jnp.zeros((groups * width, tok_rows), jnp.float32)
    for i, fact in enumerate(facts):
        spoken = jnp.where(line_fact == i, fact[None, :], spoken)
    spoken = jnp.where((lines // width)[:, None] == group_choice[None, :], spoken, 0.0)
    columns = rank[:, None] == jnp.arange(piece_width, dtype=jnp.int32)[None, :]
    told = dot(spoken.astype(jnp.bfloat16), columns.astype(jnp.bfloat16)).astype(jnp.bfloat16)

    seating = lines[:, None] == (group_choice * width + rank)[None, :]
    seated = dot(seating.astype(jnp.bfloat16), tokens) + told.astype(jnp.float32)
    seated = seated.astype(jnp.bfloat16)
    landed = exchange(seated.reshape(groups, width, piece_width), "g")

    heard = landed[:, per_group:, :width].astype(jnp.float32)
    choices = [heard[:, k].astype(jnp.int32) for k in range(2)]
    shares = [heard[:, 2 + k] + heard[:, 4 + k] for k in range(2)]
    experts = jnp.arange(members, dtype=jnp.int32)[None, :, None]
    inside = jnp.arange(width, dtype=jnp.int32)[None, :] < per_group
    chosen = [(choices[k][:, None, :] == experts) & inside[:, None, :] for k in range(2)]
    named = (chosen[0] | chosen[1]).astype(jnp.bfloat16).reshape(groups * members, width)
    after = jnp.triu(jnp.ones((width, width), jnp.bfloat16), 1)
    earlier = dot(named, after).reshape(groups, members, width)
    sources = groups // tp_count
    slots = sources * capacity
    depth = up_to(slots, TILE)
    block = jnp.arange(groups, dtype=jnp.int32)[:, None]
    targets = []
    for k in range(2):
        seat = jnp.sum(jnp.where(chosen[k], earlier, 0.0), 1).astype(jnp.int32)
        place = (block // sources * members + choices[k]) * depth
        place = place + block % sources * capacity + seat
        targets.append(jnp.where(inside, place, -1))
    places = jnp.arange(tp_count * members * depth, dtype=jnp.int32)
    flat = [t.reshape(-1) for t in targets]
    spread = (places[:, None] == flat[0][None, :]) | (places[:, None] == flat[1][None, :])
    buffer = dot(
        spread.astype(jnp.bfloat16), landed.reshape(groups * width, piece_width)
    ).astype(jnp.bfloat16)

    rows = exchange(buffer.reshape(tp_count * members, depth, piece_width), BLOCK)
    values = rows.reshape(tp_count, members * depth, piece_width).astype(jnp.float32)
    inv_rms = lax.rsqrt(jnp.sum(values * values, (0, 2)) / model_width + 1e-06)
    gains = norm_gain.reshape(tp_count, 1, piece_width)
    normed = (values * inv_rms[None, :, None] * gains).astype(jnp.bfloat16)
    normed = jnp.concatenate([normed[t] for t in range(tp_count)], 1)
    hidden = jnp.zeros((members * depth, tp_count * units), jnp.bfloat16)
    for i, parts in enumerate(ring_in):
        both = dot_parts(normed, parts)
        piece = (jax.nn.silu(both[:, :units]) * both[:, units:]).astype(jnp.bfloat16)
        owner = lax.rem(me + i, tp_count)
        hidden = lax.dynamic_update_slice_in_dim(hidden, piece, owner * units, 1)
    results = jnp.zeros((tp_count, members * depth, piece_width), jnp.bfloat16)
    for i, parts in enumerate(ring_out):
        piece = dot_parts(hidden, parts).astype(jnp.bfloat16)
        owner = lax.rem(me + i, tp_count)
        results = lax.dynamic_update_slice_in_dim(results, piece[None], owner, 0)

    returned = exchange(results.reshape(tp_count * members, depth, piece_width), BLOCK)
    returned = returned.reshape(-1, piece_width)
    combined = jnp.zeros((tok_rows, piece_width), jnp.float32)
    for k in range(2):
        back = targets[k][:, :per_group].reshape(-1)
        share = shares[k][:, :per_group].reshape(-1)
        picker = (back[:, None] == places[None, :]).astype(jnp.bfloat16)
        combined = combined + share[:, None] * dot(picker, returned)
    combined = combined.astype(jnp.bfloat16)
    home = exchange(combined.reshape(groups, per_group, piece_width), "g")
    home = home.reshape(tok_rows, piece_width)
    here = lax.axis_index("g")
    seats = jnp.arange(per_group, dtype=jnp.int32)[None, :]
    stayed = (group_choice == here)[:, None] & (rank[:, None] == seats)
    own = lax.dynamic_slice_in_dim(combined, here * per_group, per_group, 0)
    kept = dot(stayed.astype(jnp.bfloat16), own)
    slot = jnp.where(group_choice == here, -1, group_choice * per_group + rank)
    unseating = slot[:, None] == jnp.arange(tok_rows, dtype=jnp.int32)[None, :]
    return (dot(unseating.astype(jnp.bfloat16), home) + kept).astype(jnp.bfloat16)


def solution(mesh):
    groups = mesh.shape["ep"] // GROUP_SIZE
    split = Mesh(
        mesh.devices.reshape(mesh.shape["grp"], groups, GROUP_SIZE, mesh.shape["tp"]),
        ("grp", "g", "m", "tp"),
    )
    placed = (
        P(GRP_EP, "tp"),
        P(GRP_EP),
        P(GRP_EP, None),
        P(GRP_EP),
        P(GRP_EP, None),
        P(),
        P(EP, None, "tp"),
        P(EP, None, "tp"),
        P(EP, None, "tp"),
    )
    return jax.shard_map(
        layer, mesh=split, in_specs=placed, out_specs=P(GRP_EP, "tp"), check_vma=False
    )
```

```python
import jax
import jax.numpy as jnp
from jax import lax
from jax.experimental import pallas as pl
from jax.experimental.pallas import tpu as pltpu
from jax.sharding import Mesh
from jax.sharding import PartitionSpec as P


GROUP_SIZE = 8
TILE = 8
EP = ("g", "m")
GRP_EP = ("grp", "g", "m")
BLOCK = ("tp", "m")


def exchange(array, axis):
    return lax.all_to_all(array, axis, 0, 0, tiled=True)


def shifted(array, axis, by):
    length = lax.axis_size(axis)
    return lax.ppermute(array, axis, [(a, (a + by) % length) for a in range(length)])


def up_to(length, tile):
    return -(-length // tile) * tile


def around(array, axis):
    one = shifted(array, axis, 3)
    three = shifted(array, axis, 1)
    half = array.shape[0] // 2
    top = shifted(one[:half], axis, 3)
    bottom = shifted(three[half:], axis, 1)
    return [(array,), (one,), (top, bottom), (three,)]


def dot(a, b):
    return jnp.dot(a, b, preferred_element_type=jnp.float32)


def fetch(sources, slots, semaphores):
    copies = [
        pltpu.make_async_copy(source, slot, semaphores.at[i])
        for i, (source, slot) in enumerate(zip(sources, slots, strict=True))
    ]
    for copy in copies:
        copy.start()
    return copies


def gated(both, units):
    gate, up = both[:, :units], both[:, units:]
    return (gate / (1.0 + jnp.exp(-gate)) * up).astype(jnp.bfloat16)


def first_half(gains, given, gate, up, one, three, normed, hidden, rows, *scratch):
    slots, semaphores = scratch[:-1], scratch[-1]
    arrived, *copies = fetch((given, gate, up, one, three), (rows, *slots), semaphores)
    parts, _, width = rows.shape
    units = gate.shape[1]
    total = None
    arrived.wait()
    for t in range(parts):
        values = rows[t].astype(jnp.float32)
        squares = jnp.sum(values * values, -1, keepdims=True)
        total = squares if total is None else total + squares
    inv_rms = lax.rsqrt(total / (parts * width) + 1e-06)
    for t in range(parts):
        scaled = rows[t].astype(jnp.float32) * inv_rms * gains[t][None, :]
        normed[:, t * width : (t + 1) * width] = scaled.astype(jnp.bfloat16)
    copies[0].wait()
    copies[1].wait()
    both = jnp.concatenate([dot(normed[...], s[...]) for s in slots[:2]], 1)
    hidden[0] = gated(both, units)
    for i in (2, 3):
        copies[i].wait()
        hidden[i - 1] = gated(dot(normed[...], slots[i][...]), units)


def second_half(me, *refs):
    sources, results, slots = refs[:9], refs[9], refs[10:19]
    whole, semaphores = refs[19], refs[20]
    copies = fetch(sources, slots, semaphores)
    normed, hidden, in_top, in_bottom, own, one, three, out_top, out_bottom = slots
    parts, _, _ = results.shape
    units = hidden.shape[2]

    def owner(offset):
        return lax.rem(me[0] + offset, parts)

    def place(offset, piece):
        whole[:, pl.ds(pl.multiple_of(owner(offset) * units, units), units)] = piece

    def halves(whole, top, bottom):
        half = top.shape[0]
        return dot(whole[:, :half], top[...]) + dot(whole[:, half:], bottom[...])

    for copy in copies[:4]:
        copy.wait()
    for i, offset in enumerate((0, 1, 3)):
        place(offset, hidden[i])
    place(2, gated(halves(normed, in_top, in_bottom), units))
    for copy, slot, offset in zip(copies[4:7], (own, one, three), (0, 1, 3), strict=True):
        copy.wait()
        results[owner(offset)] = dot(whole[...], slot[...]).astype(results.dtype)
    copies[7].wait()
    copies[8].wait()
    results[owner(2)] = halves(whole, out_top, out_bottom).astype(results.dtype)


def expert(rows, norm_gain, gate, up, ring_in, ring_out, me):
    parts, count, width = rows.shape
    units = gate.shape[1]
    vmem = pl.BlockSpec(memory_space=pltpu.VMEM)
    hbm = pl.BlockSpec(memory_space=pltpu.HBM)
    smem = pl.BlockSpec(memory_space=pltpu.SMEM)

    def slots(arrays):
        return [pltpu.VMEM(a.shape, a.dtype) for a in arrays]

    _, (one,), far, (three,) = ring_in
    given = [rows, gate, up, one, three]
    normed, hidden = pl.pallas_call(
        first_half,
        out_shape=(
            jax.ShapeDtypeStruct((count, parts * width), jnp.bfloat16),
            jax.ShapeDtypeStruct((3, count, units), jnp.bfloat16),
        ),
        in_specs=[vmem] + [hbm] * 5,
        out_specs=(vmem, vmem),
        scratch_shapes=slots(given) + [pltpu.SemaphoreType.DMA((5,))],
        name="first_half",
    )(norm_gain.reshape(parts, width), *given)
    (own,), (one,), far_out, (three,) = ring_out
    given = [normed, hidden, *far, own, one, three, *far_out]
    return pl.pallas_call(
        second_half,
        out_shape=jax.ShapeDtypeStruct((parts, count, width), jnp.bfloat16),
        in_specs=[smem] + [hbm] * 9,
        out_specs=vmem,
        scratch_shapes=slots(given)
        + [pltpu.VMEM((count, parts * units), jnp.bfloat16), pltpu.SemaphoreType.DMA((9,))],
        name="second_half",
    )(me.reshape(1), *given)


def layer(
    tokens,
    group_choice,
    expert_choice,
    group_weight,
    expert_weight,
    norm_gain,
    w_gate,
    w_up,
    w_down,
):
    tok_rows, piece_width = tokens.shape
    groups = lax.axis_size("g")
    members = lax.axis_size("m")
    tp_count = lax.axis_size("tp")
    me = lax.axis_index("tp")
    per_group = tok_rows // groups
    mean_load = 2 * tok_rows // (groups * members)
    capacity = mean_load + min(mean_load // 2, per_group - mean_load)
    width = per_group + TILE

    ring_in = around(jnp.concatenate([w_gate[0], w_up[0]], 1), "tp")
    ring_out = around(w_down[0], "tp")

    in_group = group_choice[:, None] == jnp.arange(groups, dtype=jnp.int32)[None, :]
    before = jnp.tril(jnp.ones((tok_rows, tok_rows), jnp.bfloat16), -1)
    ranks = dot(before, in_group.astype(jnp.bfloat16))
    rank = jnp.sum(jnp.where(in_group, ranks, 0.0), 1).astype(jnp.int32)

    mixing = group_weight[:, None] * expert_weight / jnp.sum(expert_weight, -1, keepdims=True)
    coarse = lax.reduce_precision(mixing, 8, 7)
    facts = [expert_choice[:, 0].astype(jnp.float32), expert_choice[:, 1].astype(jnp.float32)]
    facts += [coarse[:, 0], coarse[:, 1]]
    facts += [mixing[:, 0] - coarse[:, 0], mixing[:, 1] - coarse[:, 1]]
    lines = jnp.arange(groups * width, dtype=jnp.int32)
    line_fact = (lines % width - per_group)[:, None]
    spoken = jnp.zeros((groups * width, tok_rows), jnp.float32)
    for i, fact in enumerate(facts):
        spoken = jnp.where(line_fact == i, fact[None, :], spoken)
    spoken = jnp.where((lines // width)[:, None] == group_choice[None, :], spoken, 0.0)
    columns = rank[:, None] == jnp.arange(piece_width, dtype=jnp.int32)[None, :]
    told = dot(spoken.astype(jnp.bfloat16), columns.astype(jnp.bfloat16)).astype(jnp.bfloat16)

    seating = lines[:, None] == (group_choice * width + rank)[None, :]
    seated = dot(seating.astype(jnp.bfloat16), tokens) + told.astype(jnp.float32)
    seated = seated.astype(jnp.bfloat16)
    landed = exchange(seated.reshape(groups, width, piece_width), "g")

    heard = landed[:, per_group:, :width].astype(jnp.float32)
    choices = [heard[:, k].astype(jnp.int32) for k in range(2)]
    shares = [heard[:, 2 + k] + heard[:, 4 + k] for k in range(2)]
    experts = jnp.arange(members, dtype=jnp.int32)[None, :, None]
    inside = jnp.arange(width, dtype=jnp.int32)[None, :] < per_group
    chosen = [(choices[k][:, None, :] == experts) & inside[:, None, :] for k in range(2)]
    named = (chosen[0] | chosen[1]).astype(jnp.bfloat16).reshape(groups * members, width)
    after = jnp.triu(jnp.ones((width, width), jnp.bfloat16), 1)
    earlier = dot(named, after).reshape(groups, members, width)
    sources = groups // tp_count
    slots = sources * capacity
    depth = up_to(slots, TILE)
    block = jnp.arange(groups, dtype=jnp.int32)[:, None]
    targets = []
    for k in range(2):
        seat = jnp.sum(jnp.where(chosen[k], earlier, 0.0), 1).astype(jnp.int32)
        place = (block // sources * members + choices[k]) * depth
        place = place + block % sources * capacity + seat
        targets.append(jnp.where(inside, place, -1))
    places = jnp.arange(tp_count * members * depth, dtype=jnp.int32)
    flat = [t.reshape(-1) for t in targets]
    spread = (places[:, None] == flat[0][None, :]) | (places[:, None] == flat[1][None, :])
    buffer = dot(
        spread.astype(jnp.bfloat16), landed.reshape(groups * width, piece_width)
    ).astype(jnp.bfloat16)

    rows = exchange(buffer.reshape(tp_count * members, depth, piece_width), BLOCK)
    rows = rows.reshape(tp_count, members * depth, piece_width)
    results = expert(rows, norm_gain, w_gate[0], w_up[0], ring_in, ring_out, me)

    returned = exchange(results.reshape(tp_count * members, depth, piece_width), BLOCK)
    returned = returned.reshape(-1, piece_width)
    combined = jnp.zeros((tok_rows, piece_width), jnp.float32)
    for k in range(2):
        back = targets[k][:, :per_group].reshape(-1)
        share = shares[k][:, :per_group].reshape(-1)
        picker = (back[:, None] == places[None, :]).astype(jnp.bfloat16)
        combined = combined + share[:, None] * dot(picker, returned)
    combined = combined.astype(jnp.bfloat16)
    home = exchange(combined.reshape(groups, per_group, piece_width), "g")
    home = home.reshape(tok_rows, piece_width)
    here = lax.axis_index("g")
    seats = jnp.arange(per_group, dtype=jnp.int32)[None, :]
    stayed = (group_choice == here)[:, None] & (rank[:, None] == seats)
    own = lax.dynamic_slice_in_dim(combined, here * per_group, per_group, 0)
    kept = dot(stayed.astype(jnp.bfloat16), own)
    slot = jnp.where(group_choice == here, -1, group_choice * per_group + rank)
    unseating = slot[:, None] == jnp.arange(tok_rows, dtype=jnp.int32)[None, :]
    return (dot(unseating.astype(jnp.bfloat16), home) + kept).astype(jnp.bfloat16)


def solution(mesh):
    groups = mesh.shape["ep"] // GROUP_SIZE
    split = Mesh(
        mesh.devices.reshape(mesh.shape["grp"], groups, GROUP_SIZE, mesh.shape["tp"]),
        ("grp", "g", "m", "tp"),
    )
    placed = (
        P(GRP_EP, "tp"),
        P(GRP_EP),
        P(GRP_EP, None),
        P(GRP_EP),
        P(GRP_EP, None),
        P(),
        P(EP, None, "tp"),
        P(EP, None, "tp"),
        P(EP, None, "tp"),
    )
    return jax.shard_map(
        layer, mesh=split, in_specs=placed, out_specs=P(GRP_EP, "tp"), check_vma=False
    )
```

```python
import jax
import jax.numpy as jnp
from jax import lax
from jax.experimental import pallas as pl
from jax.experimental.pallas import tpu as pltpu
from jax.sharding import Mesh
from jax.sharding import PartitionSpec as P


GROUP_SIZE = 8
TILE = 8
EP = ("g", "m")
GRP_EP = ("grp", "g", "m")
BLOCK = ("tp", "m")


def exchange(array, axis):
    return lax.all_to_all(array, axis, 0, 0, tiled=True)


def shifted(array, axis, by):
    length = lax.axis_size(axis)
    return lax.ppermute(array, axis, [(a, (a + by) % length) for a in range(length)])


def up_to(length, tile):
    return -(-length // tile) * tile


def ring_in(gate, up, axis):
    gate_one = shifted(gate, axis, 3)
    up_three = shifted(up, axis, 1)
    up_one = shifted(up, axis, 3)
    gate_three = shifted(gate, axis, 1)
    gate_two = shifted(gate_one, axis, 3)
    up_two = shifted(up_three, axis, 1)
    return [gate, up, gate_one, up_one, gate_two, up_two, gate_three, up_three]


def ring_out(down, axis):
    one = shifted(down, axis, 3)
    three = shifted(down, axis, 1)
    half = down.shape[0] // 2
    top = shifted(one[:half], axis, 3)
    bottom = shifted(three[half:], axis, 1)
    return [down, one, three, top, bottom]


def dot(a, b):
    return jnp.dot(a, b, preferred_element_type=jnp.float32)


def fetch(sources, slots, semaphores):
    copies = [
        pltpu.make_async_copy(source, slot, semaphores.at[i])
        for i, (source, slot) in enumerate(zip(sources, slots, strict=True))
    ]
    for copy in copies:
        copy.start()
    return copies


def to_hidden(me, gains, *refs):
    hidden, scratch = refs[9], refs[10:]
    rows, *slots = scratch[:9]
    normed, semaphores = scratch[9:]
    arrived, *copies = fetch(refs[:9], (rows, *slots), semaphores)
    parts, _, width = rows.shape
    units = slots[0].shape[1]
    total = None
    arrived.wait()
    for t in range(parts):
        values = rows[t].astype(jnp.float32)
        squares = jnp.sum(values * values, -1, keepdims=True)
        total = squares if total is None else total + squares
    inv_rms = lax.rsqrt(total / (parts * width) + 1e-06)
    for t in range(parts):
        scaled = rows[t].astype(jnp.float32) * inv_rms * gains[t][None, :]
        normed[:, t * width : (t + 1) * width] = scaled.astype(jnp.bfloat16)
    for i in range(parts):
        copies[2 * i].wait()
        copies[2 * i + 1].wait()
        gate = dot(normed[...], slots[2 * i][...])
        up = dot(normed[...], slots[2 * i + 1][...])
        piece = (gate / (1.0 + jnp.exp(-gate)) * up).astype(jnp.bfloat16)
        at = lax.rem(me[0] + i, parts) * units
        hidden[:, pl.ds(pl.multiple_of(at, units), units)] = piece


def from_hidden(me, *refs):
    results, slots, semaphores = refs[6], refs[7:13], refs[13]
    copies = fetch(refs[:6], slots, semaphores)
    hidden, own, one, three, top, bottom = slots
    parts = results.shape[0]
    copies[0].wait()
    for copy, slot, offset in zip(copies[1:4], (own, one, three), (0, 1, 3), strict=True):
        copy.wait()
        piece = dot(hidden[...], slot[...])
        results[lax.rem(me[0] + offset, parts)] = piece.astype(results.dtype)
    copies[4].wait()
    copies[5].wait()
    half = top.shape[0]
    piece = dot(hidden[:, :half], top[...]) + dot(hidden[:, half:], bottom[...])
    results[lax.rem(me[0] + 2, parts)] = piece.astype(results.dtype)


def expert(rows, norm_gain, weights_in, weights_out, me):
    parts, count, width = rows.shape
    units = weights_in[0].shape[1]
    vmem = pl.BlockSpec(memory_space=pltpu.VMEM)
    hbm = pl.BlockSpec(memory_space=pltpu.HBM)
    smem = pl.BlockSpec(memory_space=pltpu.SMEM)

    def slots(arrays):
        return [pltpu.VMEM(a.shape, a.dtype) for a in arrays]

    me = me.reshape(1)
    given = [rows, *weights_in]
    hidden = pl.pallas_call(
        to_hidden,
        out_shape=jax.ShapeDtypeStruct((count, parts * units), jnp.bfloat16),
        in_specs=[smem, vmem] + [hbm] * 9,
        out_specs=vmem,
        scratch_shapes=slots(given)
        + [pltpu.VMEM((count, parts * width), jnp.bfloat16), pltpu.SemaphoreType.DMA((9,))],
        name="to_hidden",
    )(me, norm_gain.reshape(parts, width), *given)
    given = [hidden, *weights_out]
    return pl.pallas_call(
        from_hidden,
        out_shape=jax.ShapeDtypeStruct((parts, count, width), jnp.bfloat16),
        in_specs=[smem] + [hbm] * 6,
        out_specs=vmem,
        scratch_shapes=slots(given) + [pltpu.SemaphoreType.DMA((6,))],
        name="from_hidden",
    )(me, *given)


def layer(
    tokens,
    group_choice,
    expert_choice,
    group_weight,
    expert_weight,
    norm_gain,
    w_gate,
    w_up,
    w_down,
):
    tok_rows, piece_width = tokens.shape
    groups = lax.axis_size("g")
    members = lax.axis_size("m")
    tp_count = lax.axis_size("tp")
    me = lax.axis_index("tp")
    per_group = tok_rows // groups
    mean_load = 2 * tok_rows // (groups * members)
    capacity = mean_load + min(mean_load // 2, per_group - mean_load)
    width = per_group + TILE

    weights_in = ring_in(w_gate[0], w_up[0], "tp")
    weights_out = ring_out(w_down[0], "tp")

    in_group = group_choice[:, None] == jnp.arange(groups, dtype=jnp.int32)[None, :]
    before = jnp.tril(jnp.ones((tok_rows, tok_rows), jnp.bfloat16), -1)
    ranks = dot(before, in_group.astype(jnp.bfloat16))
    rank = jnp.sum(jnp.where(in_group, ranks, 0.0), 1).astype(jnp.int32)

    mixing = group_weight[:, None] * expert_weight / jnp.sum(expert_weight, -1, keepdims=True)
    coarse = lax.reduce_precision(mixing, 8, 7)
    facts = [expert_choice[:, 0].astype(jnp.float32), expert_choice[:, 1].astype(jnp.float32)]
    facts += [coarse[:, 0], coarse[:, 1]]
    facts += [mixing[:, 0] - coarse[:, 0], mixing[:, 1] - coarse[:, 1]]
    lines = jnp.arange(groups * width, dtype=jnp.int32)
    line_fact = (lines % width - per_group)[:, None]
    spoken = jnp.zeros((groups * width, tok_rows), jnp.float32)
    for i, fact in enumerate(facts):
        spoken = jnp.where(line_fact == i, fact[None, :], spoken)
    spoken = jnp.where((lines // width)[:, None] == group_choice[None, :], spoken, 0.0)
    columns = rank[:, None] == jnp.arange(piece_width, dtype=jnp.int32)[None, :]
    told = dot(spoken.astype(jnp.bfloat16), columns.astype(jnp.bfloat16)).astype(jnp.bfloat16)

    seating = lines[:, None] == (group_choice * width + rank)[None, :]
    seated = dot(seating.astype(jnp.bfloat16), tokens) + told.astype(jnp.float32)
    seated = seated.astype(jnp.bfloat16)
    landed = exchange(seated.reshape(groups, width, piece_width), "g")

    heard = landed[:, per_group:, :width].astype(jnp.float32)
    choices = [heard[:, k].astype(jnp.int32) for k in range(2)]
    shares = [heard[:, 2 + k] + heard[:, 4 + k] for k in range(2)]
    experts = jnp.arange(members, dtype=jnp.int32)[None, :, None]
    inside = jnp.arange(width, dtype=jnp.int32)[None, :] < per_group
    chosen = [(choices[k][:, None, :] == experts) & inside[:, None, :] for k in range(2)]
    named = (chosen[0] | chosen[1]).astype(jnp.bfloat16).reshape(groups * members, width)
    after = jnp.triu(jnp.ones((width, width), jnp.bfloat16), 1)
    earlier = dot(named, after).reshape(groups, members, width)
    sources = groups // tp_count
    slots = sources * capacity
    depth = up_to(slots, TILE)
    block = jnp.arange(groups, dtype=jnp.int32)[:, None]
    targets = []
    for k in range(2):
        seat = jnp.sum(jnp.where(chosen[k], earlier, 0.0), 1).astype(jnp.int32)
        place = (block // sources * members + choices[k]) * depth
        place = place + block % sources * capacity + seat
        targets.append(jnp.where(inside, place, -1))
    places = jnp.arange(tp_count * members * depth, dtype=jnp.int32)
    flat = [t.reshape(-1) for t in targets]
    spread = (places[:, None] == flat[0][None, :]) | (places[:, None] == flat[1][None, :])
    buffer = dot(
        spread.astype(jnp.bfloat16), landed.reshape(groups * width, piece_width)
    ).astype(jnp.bfloat16)

    rows = exchange(buffer.reshape(tp_count * members, depth, piece_width), BLOCK)
    rows = rows.reshape(tp_count, members * depth, piece_width)
    results = expert(rows, norm_gain, weights_in, weights_out, me)

    returned = exchange(results.reshape(tp_count * members, depth, piece_width), BLOCK)
    returned = returned.reshape(-1, piece_width)
    combined = jnp.zeros((tok_rows, piece_width), jnp.float32)
    for k in range(2):
        back = targets[k][:, :per_group].reshape(-1)
        share = shares[k][:, :per_group].reshape(-1)
        picker = (back[:, None] == places[None, :]).astype(jnp.bfloat16)
        combined = combined + share[:, None] * dot(picker, returned)
    combined = combined.astype(jnp.bfloat16)
    home = exchange(combined.reshape(groups, per_group, piece_width), "g")
    home = home.reshape(tok_rows, piece_width)
    here = lax.axis_index("g")
    seats = jnp.arange(per_group, dtype=jnp.int32)[None, :]
    stayed = (group_choice == here)[:, None] & (rank[:, None] == seats)
    own = lax.dynamic_slice_in_dim(combined, here * per_group, per_group, 0)
    kept = dot(stayed.astype(jnp.bfloat16), own)
    slot = jnp.where(group_choice == here, -1, group_choice * per_group + rank)
    unseating = slot[:, None] == jnp.arange(tok_rows, dtype=jnp.int32)[None, :]
    return (dot(unseating.astype(jnp.bfloat16), home) + kept).astype(jnp.bfloat16)


def solution(mesh):
    groups = mesh.shape["ep"] // GROUP_SIZE
    split = Mesh(
        mesh.devices.reshape(mesh.shape["grp"], groups, GROUP_SIZE, mesh.shape["tp"]),
        ("grp", "g", "m", "tp"),
    )
    placed = (
        P(GRP_EP, "tp"),
        P(GRP_EP),
        P(GRP_EP, None),
        P(GRP_EP),
        P(GRP_EP, None),
        P(),
        P(EP, None, "tp"),
        P(EP, None, "tp"),
        P(EP, None, "tp"),
    )
    return jax.shard_map(
        layer, mesh=split, in_specs=placed, out_specs=P(GRP_EP, "tp"), check_vma=False
    )
```

```python
import functools

import jax
import jax.numpy as jnp
from jax import lax
from jax.experimental import pallas as pl
from jax.experimental.pallas import tpu as pltpu
from jax.sharding import Mesh
from jax.sharding import PartitionSpec as P


GROUP_SIZE = 8
TILE = 8
LANES = 128
EP = ("g", "m")
GRP_EP = ("grp", "g", "m")
BLOCK = ("tp", "m")


def exchange(array, axis):
    return lax.all_to_all(array, axis, 0, 0, tiled=True)


def shifted(array, axis, by):
    length = lax.axis_size(axis)
    return lax.ppermute(array, axis, [(a, (a + by) % length) for a in range(length)])


def up_to(length, tile):
    return -(-length // tile) * tile


def ring(gate, up, down, axis):
    down_one = shifted(down, axis, 3)
    down_three = shifted(down, axis, 1)
    gate_one = shifted(gate, axis, 3)
    up_three = shifted(up, axis, 1)
    up_one = shifted(up, axis, 3)
    gate_three = shifted(gate, axis, 1)
    half = down.shape[0] // 2
    top = shifted(down_one[:half], axis, 3)
    bottom = shifted(down_three[half:], axis, 1)
    gate_two = shifted(gate_one, axis, 3)
    up_two = shifted(up_three, axis, 1)
    near = [gate, up, gate_one, up_one, gate_three, up_three]
    far = [gate_two, up_two, down, down_one, down_three, top, bottom]
    return near, far


def dot(a, b):
    return jnp.dot(a, b, preferred_element_type=jnp.float32)


def fetch(sources, slots, semaphores):
    copies = [
        pltpu.make_async_copy(source, slot, semaphores.at[i])
        for i, (source, slot) in enumerate(zip(sources, slots, strict=True))
    ]
    for copy in copies:
        copy.start()
    return copies


def iota(shape, dim):
    return lax.broadcasted_iota(jnp.int32, shape, dim)


def ones(condition):
    return jnp.where(condition, 1.0, 0.0).astype(jnp.bfloat16)


def depart(group, choice, group_share, expert_share, tokens, blocks, ranks):
    groups, _, lanes = blocks.shape
    count, width = tokens.shape
    chunks, per_group = width // lanes, count // groups
    group = group[...]
    member = group == iota((groups, count), 0)
    earlier = dot(ones(member), ones(iota((count, count), 0) < iota((count, count), 1)))
    rank = jnp.sum(jnp.where(member, earlier, 0.0), 0, keepdims=True).astype(jnp.int32)
    ranks[...] = rank
    seating = ones(iota((count, count), 0) == group * per_group + rank)
    seated = dot(seating, tokens[...]).astype(jnp.bfloat16)
    mixing = group_share[...] * expert_share[...]
    mixing = mixing / jnp.sum(expert_share[...], 0, keepdims=True)
    coarse = mixing.astype(jnp.bfloat16).astype(jnp.float32)
    fine = mixing - coarse
    choice = choice[...].astype(jnp.float32)
    facts = jnp.zeros((TILE, count), jnp.float32)
    for i, pair in enumerate((choice, coarse, fine)):
        for k in range(2):
            facts = jnp.where(iota((TILE, count), 0) == 2 * i + k, pair[k : k + 1], facts)
    spoken = [jnp.where(group == g, facts, 0.0) for g in range(groups)]
    spoken = jnp.concatenate(spoken, 0).astype(jnp.bfloat16)
    columns = ones(iota((lanes, count), 0) == rank)
    told = lax.dot_general(
        spoken, columns, (((1,), (1,)), ((), ())), preferred_element_type=jnp.float32
    ).astype(jnp.bfloat16)
    for g in range(groups):
        for c in range(chunks):
            piece = seated[g * per_group : (g + 1) * per_group, c * lanes : (c + 1) * lanes]
            blocks[g, c * per_group : (c + 1) * per_group, :] = piece
        blocks[g, chunks * per_group :, :] = told[g * TILE : (g + 1) * TILE]


def arrive(capacity, landed, buffer, places, shares, seats):
    groups, lines, lanes = landed.shape
    parts, count, width = buffer.shape
    chunks = width // lanes
    per_group = (lines - TILE) // chunks
    members = GROUP_SIZE
    depth = count // members
    sources = groups // parts
    told = landed[:, chunks * per_group :, :].astype(jnp.float32)
    told = told.reshape(groups * TILE, lanes).astype(jnp.bfloat16)
    wanted = (6 * groups, groups * TILE)
    row = iota(wanted, 0)
    pick = iota(wanted, 1) == lax.rem(row, groups) * TILE + lax.div(row, groups)
    heard = dot(ones(pick), told)
    facts = [heard[i * groups : (i + 1) * groups] for i in range(6)]
    choices = [fact.astype(jnp.int32) for fact in facts[:2]]
    inside = iota((groups, lanes), 1) < per_group
    named = []
    for e in range(members):
        hit = (choices[0] == e) | (choices[1] == e)
        named.append(jnp.where(hit & inside, 1.0, 0.0))
    named = jnp.concatenate(named, 0).astype(jnp.bfloat16)
    earlier = dot(named, ones(iota((lanes, lanes), 0) < iota((lanes, lanes), 1)))
    source = iota((groups, lanes), 0)
    local = []
    for k in range(2):
        seat = jnp.zeros((groups, lanes), jnp.float32)
        for e in range(members):
            seat = jnp.where(choices[k] == e, earlier[e * groups : (e + 1) * groups], seat)
        place = choices[k] * depth + lax.rem(source, sources) * capacity + seat.astype(jnp.int32)
        local.append(jnp.where(inside, place, -1))
        places[k] = jnp.where(inside, lax.div(source, sources) * count + place, -1)
        shares[k] = facts[2 + k] + facts[4 + k]
    for g in range(groups):
        seats[g, per_group:, :] = jnp.zeros((lanes - per_group, width), jnp.bfloat16)
        for c in range(chunks):
            piece = landed[g, c * per_group : (c + 1) * per_group, :]
            seats[g, :per_group, c * lanes : (c + 1) * lanes] = piece
    rows = iota((count, lanes), 0)
    for p in range(parts):
        spread = []
        for g in range(p * sources, (p + 1) * sources):
            hit = (rows == local[0][g : g + 1]) | (rows == local[1][g : g + 1])
            spread.append(ones(hit))
        spread = jnp.concatenate(spread, 1)
        held = seats[p * sources : (p + 1) * sources].reshape(sources * lanes, width)
        buffer[p] = dot(spread, held).astype(jnp.bfloat16)


def gate_up(normed, gate, up):
    gate, up = dot(normed[...], gate[...]), dot(normed[...], up[...])
    return (gate / (1.0 + jnp.exp(-gate)) * up).astype(jnp.bfloat16)


def columns_of(me, offset, parts, units):
    return pl.ds(pl.multiple_of(lax.rem(me[0] + offset, parts) * units, units), units)


def first_half(me, gains, *refs):
    given, (normed, hidden), (rows, *slots), semaphores = refs[:7], refs[7:9], refs[9:16], refs[16]
    arrived, *copies = fetch(given, (rows, *slots), semaphores)
    parts, _, width = rows.shape
    units = slots[0].shape[1]
    total = None
    arrived.wait()
    for t in range(parts):
        values = rows[t].astype(jnp.float32)
        squares = jnp.sum(values * values, -1, keepdims=True)
        total = squares if total is None else total + squares
    inv_rms = lax.rsqrt(total / (parts * width) + 1e-06)
    for t in range(parts):
        scaled = rows[t].astype(jnp.float32) * inv_rms * gains[t][None, :]
        normed[:, t * width : (t + 1) * width] = scaled.astype(jnp.bfloat16)
    for i, offset in enumerate((0, 1, 3)):
        copies[2 * i].wait()
        copies[2 * i + 1].wait()
        piece = gate_up(normed, slots[2 * i], slots[2 * i + 1])
        hidden[:, columns_of(me, offset, parts, units)] = piece


def second_half(me, *refs):
    given, results, slots, semaphores = refs[:9], refs[9], refs[10:19], refs[19]
    copies = fetch(given, slots, semaphores)
    normed, hidden, gate, up, own, one, three, top, bottom = slots
    parts, units = results.shape[0], gate.shape[1]
    for copy in copies[:4]:
        copy.wait()
    hidden[:, columns_of(me, 2, parts, units)] = gate_up(normed, gate, up)
    for copy, slot, offset in zip(copies[4:7], (own, one, three), (0, 1, 3), strict=True):
        copy.wait()
        piece = dot(hidden[...], slot[...])
        results[lax.rem(me[0] + offset, parts)] = piece.astype(results.dtype)
    copies[7].wait()
    copies[8].wait()
    half = top.shape[0]
    piece = dot(hidden[:, :half], top[...]) + dot(hidden[:, half:], bottom[...])
    results[lax.rem(me[0] + 2, parts)] = piece.astype(results.dtype)


VMEM = pl.BlockSpec(memory_space=pltpu.VMEM)
HBM = pl.BlockSpec(memory_space=pltpu.HBM)
SMEM = pl.BlockSpec(memory_space=pltpu.SMEM)


def shaped(shape, dtype=jnp.bfloat16):
    return jax.ShapeDtypeStruct(shape, dtype)


def slots_for(arrays):
    slots = [pltpu.VMEM(a.shape, a.dtype) for a in arrays]
    return slots + [pltpu.SemaphoreType.DMA((len(arrays),))]


def expert(rows, norm_gain, near, far, me):
    parts, count, width = rows.shape
    units = near[0].shape[1]
    me = me.reshape(1)
    given = [rows, *near]
    normed, hidden = pl.pallas_call(
        first_half,
        out_shape=(shaped((count, parts * width)), shaped((count, parts * units))),
        in_specs=[SMEM, VMEM] + [HBM] * len(given),
        out_specs=(VMEM, VMEM),
        scratch_shapes=slots_for(given),
        name="first_half",
    )(me, norm_gain.reshape(parts, width), *given)
    given = [normed, hidden, *far]
    return pl.pallas_call(
        second_half,
        out_shape=shaped((parts, count, width)),
        in_specs=[SMEM] + [HBM] * len(given),
        out_specs=VMEM,
        scratch_shapes=slots_for(given),
        name="second_half",
    )(me, *given)


def layer(
    tokens,
    group_choice,
    expert_choice,
    group_weight,
    expert_weight,
    norm_gain,
    w_gate,
    w_up,
    w_down,
):
    tok_rows, piece_width = tokens.shape
    groups = lax.axis_size("g")
    members = lax.axis_size("m")
    tp_count = lax.axis_size("tp")
    me = lax.axis_index("tp")
    per_group = tok_rows // groups
    mean_load = 2 * tok_rows // (groups * members)
    capacity = mean_load + min(mean_load // 2, per_group - mean_load)
    chunks = piece_width // LANES
    depth = up_to(groups // tp_count * capacity, TILE)

    near, far = ring(w_gate[0], w_up[0], w_down[0], "tp")

    blocks, rank = pl.pallas_call(
        depart,
        out_shape=(
            shaped((groups, chunks * per_group + TILE, LANES)),
            shaped((1, tok_rows), jnp.int32),
        ),
        in_specs=[VMEM] * 5,
        out_specs=(VMEM, VMEM),
        name="depart",
    )(group_choice[None], expert_choice.T, group_weight[None], expert_weight.T, tokens)
    rank = rank[0]
    landed = exchange(blocks, "g")

    facts_shape = (2, groups, LANES)
    buffer, targets, shares = pl.pallas_call(
        functools.partial(arrive, capacity),
        out_shape=(
            shaped((tp_count, members * depth, piece_width)),
            shaped(facts_shape, jnp.int32),
            shaped(facts_shape, jnp.float32),
        ),
        in_specs=[VMEM],
        out_specs=(VMEM, VMEM, VMEM),
        scratch_shapes=[pltpu.VMEM((groups, LANES, piece_width), jnp.bfloat16)],
        name="arrive",
    )(landed)
    rows = exchange(buffer.reshape(tp_count * members, depth, piece_width), BLOCK)
    rows = rows.reshape(tp_count, members * depth, piece_width)
    results = expert(rows, norm_gain, near, far, me)

    returned = exchange(results.reshape(tp_count * members, depth, piece_width), BLOCK)
    returned = returned.reshape(-1, piece_width)
    places = jnp.arange(returned.shape[0], dtype=jnp.int32)
    combined = jnp.zeros((tok_rows, piece_width), jnp.float32)
    for k in range(2):
        back = targets[k][:, :per_group].reshape(-1)
        share = shares[k][:, :per_group].reshape(-1)
        picker = (back[:, None] == places[None, :]).astype(jnp.bfloat16)
        combined = combined + share[:, None] * dot(picker, returned)
    combined = combined.astype(jnp.bfloat16)
    home = exchange(combined.reshape(groups, per_group, piece_width), "g")
    home = home.reshape(tok_rows, piece_width)
    here = lax.axis_index("g")
    seats = jnp.arange(per_group, dtype=jnp.int32)[None, :]
    stayed = (group_choice == here)[:, None] & (rank[:, None] == seats)
    own = lax.dynamic_slice_in_dim(combined, here * per_group, per_group, 0)
    kept = dot(stayed.astype(jnp.bfloat16), own)
    slot = jnp.where(group_choice == here, -1, group_choice * per_group + rank)
    unseating = slot[:, None] == jnp.arange(tok_rows, dtype=jnp.int32)[None, :]
    return (dot(unseating.astype(jnp.bfloat16), home) + kept).astype(jnp.bfloat16)


def solution(mesh):
    groups = mesh.shape["ep"] // GROUP_SIZE
    split = Mesh(
        mesh.devices.reshape(mesh.shape["grp"], groups, GROUP_SIZE, mesh.shape["tp"]),
        ("grp", "g", "m", "tp"),
    )
    placed = (
        P(GRP_EP, "tp"),
        P(GRP_EP),
        P(GRP_EP, None),
        P(GRP_EP),
        P(GRP_EP, None),
        P(),
        P(EP, None, "tp"),
        P(EP, None, "tp"),
        P(EP, None, "tp"),
    )
    return jax.shard_map(
        layer, mesh=split, in_specs=placed, out_specs=P(GRP_EP, "tp"), check_vma=False
    )
```

```python
import functools

import jax
import jax.numpy as jnp
from jax import lax
from jax.experimental import pallas as pl
from jax.experimental.pallas import tpu as pltpu
from jax.sharding import Mesh
from jax.sharding import PartitionSpec as P


GROUP_SIZE = 8
TILE = 8
LANES = 128
EP = ("g", "m")
GRP_EP = ("grp", "g", "m")
BLOCK = ("tp", "m")


def exchange(array, axis):
    return lax.all_to_all(array, axis, 0, 0, tiled=True)


def shifted(array, axis, by):
    length = lax.axis_size(axis)
    return lax.ppermute(array, axis, [(a, (a + by) % length) for a in range(length)])


def up_to(length, tile):
    return -(-length // tile) * tile


def around(array, axis):
    one = shifted(array, axis, 3)
    three = shifted(array, axis, 1)
    half = array.shape[0] // 2
    top = shifted(one[:half], axis, 3)
    bottom = shifted(three[half:], axis, 1)
    return [one, three], [top, bottom]


def dot(a, b):
    return jnp.dot(a, b, preferred_element_type=jnp.float32)


def fetch(sources, slots, semaphores):
    copies = [
        pltpu.make_async_copy(source, slot, semaphores.at[i])
        for i, (source, slot) in enumerate(zip(sources, slots, strict=True))
    ]
    for copy in copies:
        copy.start()
    return copies


def gated(both, units):
    gate, up = both[:, :units], both[:, units:]
    return (gate / (1.0 + jnp.exp(-gate)) * up).astype(jnp.bfloat16)


def iota(shape, dim):
    return lax.broadcasted_iota(jnp.int32, shape, dim)


def ones(condition):
    return jnp.where(condition, 1.0, 0.0).astype(jnp.bfloat16)


def depart(group, choice, group_share, expert_share, tokens, blocks, ranks):
    groups, _, lanes = blocks.shape
    count, width = tokens.shape
    chunks, per_group = width // lanes, count // groups
    group = group[...].reshape(1, count)
    member = group == iota((groups, count), 0)
    earlier = dot(ones(member), ones(iota((count, count), 0) < iota((count, count), 1)))
    rank = jnp.sum(jnp.where(member, earlier, 0.0), 0, keepdims=True).astype(jnp.int32)
    ranks[...] = rank
    seating = ones(iota((count, count), 0) == group * per_group + rank)
    seated = dot(seating, tokens[...]).astype(jnp.bfloat16)
    mixing = group_share[...].reshape(1, count) * expert_share[...]
    mixing = mixing / jnp.sum(expert_share[...], 0, keepdims=True)
    coarse = mixing.astype(jnp.bfloat16).astype(jnp.float32)
    fine = mixing - coarse
    choice = choice[...].astype(jnp.float32)
    facts = jnp.zeros((TILE, count), jnp.float32)
    for i, pair in enumerate((choice, coarse, fine)):
        for k in range(2):
            facts = jnp.where(iota((TILE, count), 0) == 2 * i + k, pair[k : k + 1], facts)
    spoken = [jnp.where(group == g, facts, 0.0) for g in range(groups)]
    spoken = jnp.concatenate(spoken, 0).astype(jnp.bfloat16)
    columns = ones(iota((lanes, count), 0) == rank)
    told = lax.dot_general(
        spoken, columns, (((1,), (1,)), ((), ())), preferred_element_type=jnp.float32
    ).astype(jnp.bfloat16)
    for g in range(groups):
        for c in range(chunks):
            piece = seated[g * per_group : (g + 1) * per_group, c * lanes : (c + 1) * lanes]
            blocks[g, c * per_group : (c + 1) * per_group, :] = piece
        blocks[g, chunks * per_group :, :] = told[g * TILE : (g + 1) * TILE]


def arrive(capacity, landed, buffer, places, shares, seats):
    groups, lines, lanes = landed.shape
    parts, count, width = buffer.shape
    chunks = width // lanes
    per_group = (lines - TILE) // chunks
    members = GROUP_SIZE
    depth = count // members
    sources = groups // parts
    told = landed[:, chunks * per_group :, :].astype(jnp.float32)
    told = told.reshape(groups * TILE, lanes).astype(jnp.bfloat16)
    wanted = (6 * groups, groups * TILE)
    row = iota(wanted, 0)
    pick = iota(wanted, 1) == lax.rem(row, groups) * TILE + lax.div(row, groups)
    heard = dot(ones(pick), told)
    facts = [heard[i * groups : (i + 1) * groups] for i in range(6)]
    choices = [fact.astype(jnp.int32) for fact in facts[:2]]
    inside = iota((groups, lanes), 1) < per_group
    named = []
    for e in range(members):
        hit = (choices[0] == e) | (choices[1] == e)
        named.append(jnp.where(hit & inside, 1.0, 0.0))
    named = jnp.concatenate(named, 0).astype(jnp.bfloat16)
    earlier = dot(named, ones(iota((lanes, lanes), 0) < iota((lanes, lanes), 1)))
    source = iota((groups, lanes), 0)
    local = []
    for k in range(2):
        seat = jnp.zeros((groups, lanes), jnp.float32)
        for e in range(members):
            seat = jnp.where(choices[k] == e, earlier[e * groups : (e + 1) * groups], seat)
        place = choices[k] * depth + lax.rem(source, sources) * capacity + seat.astype(jnp.int32)
        local.append(jnp.where(inside, place, -1))
        places[k] = jnp.where(inside, lax.div(source, sources) * count + place, -1)
        shares[k] = facts[2 + k] + facts[4 + k]
    for g in range(groups):
        seats[g, per_group:, :] = jnp.zeros((lanes - per_group, width), jnp.bfloat16)
        for c in range(chunks):
            piece = landed[g, c * per_group : (c + 1) * per_group, :]
            seats[g, :per_group, c * lanes : (c + 1) * lanes] = piece
    rows = iota((count, lanes), 0)
    for p in range(parts):
        spread = []
        for g in range(p * sources, (p + 1) * sources):
            hit = (rows == local[0][g : g + 1]) | (rows == local[1][g : g + 1])
            spread.append(ones(hit))
        spread = jnp.concatenate(spread, 1)
        held = seats[p * sources : (p + 1) * sources].reshape(sources * lanes, width)
        buffer[p] = dot(spread, held).astype(jnp.bfloat16)


def gated(gate, up):
    return (gate / (1.0 + jnp.exp(-gate)) * up).astype(jnp.bfloat16)


def place(hidden, me, offset, parts, piece):
    units = piece.shape[1]
    at = pl.multiple_of(lax.rem(me[0] + offset, parts) * units, units)
    hidden[:, pl.ds(at, units)] = piece


def by_halves(whole, top, bottom):
    half = top.shape[0]
    return dot(whole[:, :half], top[...]) + dot(whole[:, half:], bottom[...])


def first_half(me, gains, *refs):
    given, (normed, hidden), (rows, *slots), semaphores = refs[:5], refs[5:7], refs[7:12], refs[12]
    gate, up, one, three = slots
    arrived, *copies = fetch(given, (rows, *slots), semaphores)
    parts, _, width = rows.shape
    units = gate.shape[1]
    total = None
    arrived.wait()
    for t in range(parts):
        values = rows[t].astype(jnp.float32)
        squares = jnp.sum(values * values, -1, keepdims=True)
        total = squares if total is None else total + squares
    inv_rms = lax.rsqrt(total / (parts * width) + 1e-06)
    for t in range(parts):
        scaled = rows[t].astype(jnp.float32) * inv_rms * gains[t][None, :]
        normed[:, t * width : (t + 1) * width] = scaled.astype(jnp.bfloat16)
    copies[0].wait()
    copies[1].wait()
    piece = gated(dot(normed[...], gate[...]), dot(normed[...], up[...]))
    place(hidden, me, 0, parts, piece)
    for copy, slot, offset in zip(copies[2:], (one, three), (1, 3), strict=True):
        copy.wait()
        both = dot(normed[...], slot[...])
        place(hidden, me, offset, parts, gated(both[:, :units], both[:, units:]))


def second_half(me, *refs):
    given, results, slots, semaphores = refs[:9], refs[9], refs[10:19], refs[19]
    copies = fetch(given, slots, semaphores)
    normed, hidden, top, bottom, own, one, three, down_top, down_bottom = slots
    parts = results.shape[0]
    units = hidden.shape[1] // parts
    for copy in copies[:4]:
        copy.wait()
    both = by_halves(normed, top, bottom)
    place(hidden, me, 2, parts, gated(both[:, :units], both[:, units:]))
    for copy, slot, offset in zip(copies[4:7], (own, one, three), (0, 1, 3), strict=True):
        copy.wait()
        owner = lax.rem(me[0] + offset, parts)
        results[owner] = dot(hidden[...], slot[...]).astype(results.dtype)
    copies[7].wait()
    copies[8].wait()
    owner = lax.rem(me[0] + 2, parts)
    results[owner] = by_halves(hidden, down_top, down_bottom).astype(results.dtype)


VMEM = pl.BlockSpec(memory_space=pltpu.VMEM)
HBM = pl.BlockSpec(memory_space=pltpu.HBM)
SMEM = pl.BlockSpec(memory_space=pltpu.SMEM)


def shaped(shape, dtype=jnp.bfloat16):
    return jax.ShapeDtypeStruct(shape, dtype)


def slots_for(arrays):
    return [pltpu.VMEM(a.shape, a.dtype) for a in arrays]


def expert(rows, norm_gain, gate, up, down, gate_up_ring, down_ring, me):
    parts, count, width = rows.shape
    units = gate.shape[1]
    me = me.reshape(1)
    near, far = gate_up_ring
    given = [rows, gate, up, *near]
    normed, hidden = pl.pallas_call(
        first_half,
        out_shape=(shaped((count, parts * width)), shaped((count, parts * units))),
        in_specs=[SMEM, VMEM] + [HBM] * len(given),
        out_specs=(VMEM, VMEM),
        scratch_shapes=slots_for(given) + [pltpu.SemaphoreType.DMA((len(given),))],
        name="first_half",
    )(me, norm_gain.reshape(parts, width), *given)
    near, far_down = down_ring
    given = [normed, hidden, *far, down, *near, *far_down]
    return pl.pallas_call(
        second_half,
        out_shape=shaped((parts, count, width)),
        in_specs=[SMEM] + [HBM] * len(given),
        out_specs=VMEM,
        scratch_shapes=slots_for(given) + [pltpu.SemaphoreType.DMA((len(given),))],
        name="second_half",
    )(me, *given)


def layer(
    tokens,
    group_choice,
    expert_choice,
    group_weight,
    expert_weight,
    norm_gain,
    w_gate,
    w_up,
    w_down,
):
    tok_rows, piece_width = tokens.shape
    groups = lax.axis_size("g")
    members = lax.axis_size("m")
    tp_count = lax.axis_size("tp")
    me = lax.axis_index("tp")
    per_group = tok_rows // groups
    mean_load = 2 * tok_rows // (groups * members)
    capacity = mean_load + min(mean_load // 2, per_group - mean_load)
    chunks = piece_width // LANES
    depth = up_to(groups // tp_count * capacity, TILE)

    gate_up_ring = around(jnp.concatenate([w_gate[0], w_up[0]], 1), "tp")
    down_ring = around(w_down[0], "tp")

    blocks, rank = pl.pallas_call(
        depart,
        out_shape=(
            shaped((groups, chunks * per_group + TILE, LANES)),
            shaped((1, tok_rows), jnp.int32),
        ),
        in_specs=[VMEM] * 5,
        out_specs=(VMEM, VMEM),
        name="depart",
    )(group_choice, expert_choice.T, group_weight, expert_weight.T, tokens)
    rank = rank[0]
    landed = exchange(blocks, "g")

    facts_shape = (2, groups, LANES)
    buffer, targets, shares = pl.pallas_call(
        functools.partial(arrive, capacity),
        out_shape=(
            shaped((tp_count, members * depth, piece_width)),
            shaped(facts_shape, jnp.int32),
            shaped(facts_shape, jnp.float32),
        ),
        in_specs=[VMEM],
        out_specs=(VMEM, VMEM, VMEM),
        scratch_shapes=[pltpu.VMEM((groups, LANES, piece_width), jnp.bfloat16)],
        name="arrive",
    )(landed)
    rows = exchange(buffer.reshape(tp_count * members, depth, piece_width), BLOCK)
    rows = rows.reshape(tp_count, members * depth, piece_width)
    results = expert(
        rows, norm_gain, w_gate[0], w_up[0], w_down[0], gate_up_ring, down_ring, me
    )

    returned = exchange(results.reshape(tp_count * members, depth, piece_width), BLOCK)
    returned = returned.reshape(-1, piece_width)
    places = jnp.arange(returned.shape[0], dtype=jnp.int32)
    combined = jnp.zeros((tok_rows, piece_width), jnp.float32)
    for k in range(2):
        back = targets[k][:, :per_group].reshape(-1)
        share = shares[k][:, :per_group].reshape(-1)
        picker = (back[:, None] == places[None, :]).astype(jnp.bfloat16)
        combined = combined + share[:, None] * dot(picker, returned)
    combined = combined.astype(jnp.bfloat16)
    home = exchange(combined.reshape(groups, per_group, piece_width), "g")
    home = home.reshape(tok_rows, piece_width)
    here = lax.axis_index("g")
    seats = jnp.arange(per_group, dtype=jnp.int32)[None, :]
    stayed = (group_choice == here)[:, None] & (rank[:, None] == seats)
    own = lax.dynamic_slice_in_dim(combined, here * per_group, per_group, 0)
    kept = dot(stayed.astype(jnp.bfloat16), own)
    slot = jnp.where(group_choice == here, -1, group_choice * per_group + rank)
    unseating = slot[:, None] == jnp.arange(tok_rows, dtype=jnp.int32)[None, :]
    return (dot(unseating.astype(jnp.bfloat16), home) + kept).astype(jnp.bfloat16)


def solution(mesh):
    groups = mesh.shape["ep"] // GROUP_SIZE
    split = Mesh(
        mesh.devices.reshape(mesh.shape["grp"], groups, GROUP_SIZE, mesh.shape["tp"]),
        ("grp", "g", "m", "tp"),
    )
    placed = (
        P(GRP_EP, "tp"),
        P(GRP_EP),
        P(GRP_EP, None),
        P(GRP_EP),
        P(GRP_EP, None),
        P(),
        P(EP, None, "tp"),
        P(EP, None, "tp"),
        P(EP, None, "tp"),
    )
    return jax.shard_map(
        layer, mesh=split, in_specs=placed, out_specs=P(GRP_EP, "tp"), check_vma=False
    )
```

```python
import functools

import jax
import jax.numpy as jnp
from jax import lax
from jax.experimental import pallas as pl
from jax.experimental.pallas import tpu as pltpu
from jax.sharding import Mesh
from jax.sharding import PartitionSpec as P


GROUP_SIZE = 8
TILE = 8
LANES = 128
EP = ("g", "m")
GRP_EP = ("grp", "g", "m")
BLOCK = ("tp", "m")


def exchange(array, axis):
    return lax.all_to_all(array, axis, 0, 0, tiled=True)


def shifted(array, axis, by):
    length = lax.axis_size(axis)
    return lax.ppermute(array, axis, [(a, (a + by) % length) for a in range(length)])


def up_to(length, tile):
    return -(-length // tile) * tile


def around(array, axis):
    one = shifted(array, axis, 3)
    three = shifted(array, axis, 1)
    half = array.shape[0] // 2
    top = shifted(one[:half], axis, 3)
    bottom = shifted(three[half:], axis, 1)
    return [one, three], [top, bottom]


def dot(a, b):
    return jnp.dot(a, b, preferred_element_type=jnp.float32)


def fetch(sources, slots, semaphores):
    copies = [
        pltpu.make_async_copy(source, slot, semaphores.at[i])
        for i, (source, slot) in enumerate(zip(sources, slots, strict=True))
    ]
    for copy in copies:
        copy.start()
    return copies


def gated(both, units):
    gate, up = both[:, :units], both[:, units:]
    return (gate / (1.0 + jnp.exp(-gate)) * up).astype(jnp.bfloat16)


def iota(shape, dim):
    return lax.broadcasted_iota(jnp.int32, shape, dim)


def ones(condition):
    return jnp.where(condition, 1.0, 0.0).astype(jnp.bfloat16)


def depart(group, choice, group_share, expert_share, tokens, blocks, ranks):
    groups, _, lanes = blocks.shape
    count, width = tokens.shape
    chunks, per_group = width // lanes, count // groups
    group = group[...].reshape(1, count)
    member = group == iota((groups, count), 0)
    earlier = dot(ones(member), ones(iota((count, count), 0) < iota((count, count), 1)))
    rank = jnp.sum(jnp.where(member, earlier, 0.0), 0, keepdims=True).astype(jnp.int32)
    ranks[...] = rank
    seating = ones(iota((count, count), 0) == group * per_group + rank)
    seated = dot(seating, tokens[...]).astype(jnp.bfloat16)
    mixing = group_share[...].reshape(1, count) * expert_share[...]
    mixing = mixing / jnp.sum(expert_share[...], 0, keepdims=True)
    coarse = mixing.astype(jnp.bfloat16).astype(jnp.float32)
    fine = mixing - coarse
    choice = choice[...].astype(jnp.float32)
    facts = jnp.zeros((TILE, count), jnp.float32)
    for i, pair in enumerate((choice, coarse, fine)):
        for k in range(2):
            facts = jnp.where(iota((TILE, count), 0) == 2 * i + k, pair[k : k + 1], facts)
    spoken = [jnp.where(group == g, facts, 0.0) for g in range(groups)]
    spoken = jnp.concatenate(spoken, 0).astype(jnp.bfloat16)
    columns = ones(iota((lanes, count), 0) == rank)
    told = lax.dot_general(
        spoken, columns, (((1,), (1,)), ((), ())), preferred_element_type=jnp.float32
    ).astype(jnp.bfloat16)
    for g in range(groups):
        for c in range(chunks):
            piece = seated[g * per_group : (g + 1) * per_group, c * lanes : (c + 1) * lanes]
            blocks[g, c * per_group : (c + 1) * per_group, :] = piece
        blocks[g, chunks * per_group :, :] = told[g * TILE : (g + 1) * TILE]


def arrive(capacity, landed, buffer, places, shares, seats):
    groups, lines, lanes = landed.shape
    parts, count, width = buffer.shape
    chunks = width // lanes
    per_group = (lines - TILE) // chunks
    members = GROUP_SIZE
    depth = count // members
    sources = groups // parts
    told = landed[:, chunks * per_group :, :].astype(jnp.float32)
    told = told.reshape(groups * TILE, lanes).astype(jnp.bfloat16)
    wanted = (6 * groups, groups * TILE)
    row = iota(wanted, 0)
    pick = iota(wanted, 1) == lax.rem(row, groups) * TILE + lax.div(row, groups)
    heard = dot(ones(pick), told)
    facts = [heard[i * groups : (i + 1) * groups] for i in range(6)]
    choices = [fact.astype(jnp.int32) for fact in facts[:2]]
    inside = iota((groups, lanes), 1) < per_group
    named = []
    for e in range(members):
        hit = (choices[0] == e) | (choices[1] == e)
        named.append(jnp.where(hit & inside, 1.0, 0.0))
    named = jnp.concatenate(named, 0).astype(jnp.bfloat16)
    earlier = dot(named, ones(iota((lanes, lanes), 0) < iota((lanes, lanes), 1)))
    source = iota((groups, lanes), 0)
    local = []
    for k in range(2):
        seat = jnp.zeros((groups, lanes), jnp.float32)
        for e in range(members):
            seat = jnp.where(choices[k] == e, earlier[e * groups : (e + 1) * groups], seat)
        place = choices[k] * depth + lax.rem(source, sources) * capacity + seat.astype(jnp.int32)
        local.append(jnp.where(inside, place, -1))
        places[k] = jnp.where(inside, lax.div(source, sources) * count + place, -1)
        shares[k] = facts[2 + k] + facts[4 + k]
    for g in range(groups):
        seats[g, per_group:, :] = jnp.zeros((lanes - per_group, width), jnp.bfloat16)
        for c in range(chunks):
            piece = landed[g, c * per_group : (c + 1) * per_group, :]
            seats[g, :per_group, c * lanes : (c + 1) * lanes] = piece
    rows = iota((count, lanes), 0)
    for p in range(parts):
        spread = []
        for g in range(p * sources, (p + 1) * sources):
            hit = (rows == local[0][g : g + 1]) | (rows == local[1][g : g + 1])
            spread.append(ones(hit))
        spread = jnp.concatenate(spread, 1)
        held = seats[p * sources : (p + 1) * sources].reshape(sources * lanes, width)
        buffer[p] = dot(spread, held).astype(jnp.bfloat16)


def gated(gate, up):
    return (gate / (1.0 + jnp.exp(-gate)) * up).astype(jnp.bfloat16)


def place(hidden, me, offset, parts, piece):
    units = piece.shape[1]
    at = pl.multiple_of(lax.rem(me[0] + offset, parts) * units, units)
    hidden[:, pl.ds(at, units)] = piece


def by_halves(whole, top, bottom):
    half = top.shape[0]
    return dot(whole[:, :half], top[...]) + dot(whole[:, half:], bottom[...])


def main_part(me, gains, *refs):
    given, (hidden_out, results), (rows, *slots) = refs[:10], refs[10:12], refs[12:22]
    normed, hidden, pieces, semaphores, leaving = refs[22:]
    gate, up, one, three, top, bottom, *down = slots
    arrived, *copies = fetch(given, (rows, *slots), semaphores)
    parts, _, width = rows.shape
    units = gate.shape[1]
    total = None
    arrived.wait()
    for t in range(parts):
        values = rows[t].astype(jnp.float32)
        squares = jnp.sum(values * values, -1, keepdims=True)
        total = squares if total is None else total + squares
    inv_rms = lax.rsqrt(total / (parts * width) + 1e-06)
    for t in range(parts):
        scaled = rows[t].astype(jnp.float32) * inv_rms * gains[t][None, :]
        normed[:, t * width : (t + 1) * width] = scaled.astype(jnp.bfloat16)
    copies[0].wait()
    copies[1].wait()
    piece = gated(dot(normed[...], gate[...]), dot(normed[...], up[...]))
    place(hidden, me, 0, parts, piece)
    for copy, slot, offset in zip(copies[2:4], (one, three), (1, 3), strict=True):
        copy.wait()
        both = dot(normed[...], slot[...])
        place(hidden, me, offset, parts, gated(both[:, :units], both[:, units:]))
    copies[4].wait()
    copies[5].wait()
    both = by_halves(normed, top, bottom)
    place(hidden, me, 2, parts, gated(both[:, :units], both[:, units:]))
    out = [pltpu.make_async_copy(hidden, hidden_out, leaving.at[3])]
    out[0].start()
    for i, offset in enumerate((0, 1, 3)):
        copies[6 + i].wait()
        pieces[i] = dot(hidden[...], down[i][...]).astype(pieces.dtype)
        owner = lax.rem(me[0] + offset, parts)
        out.append(pltpu.make_async_copy(pieces.at[i], results.at[owner], leaving.at[i]))
        out[-1].start()
    for copy in out:
        copy.wait()


def last_part(me, *refs):
    given, results, slots, piece, semaphores = refs[:3], refs[4], refs[5:8], refs[8], refs[9]
    for copy in fetch(given, slots, semaphores):
        copy.wait()
    hidden, top, bottom = slots
    piece[...] = by_halves(hidden, top, bottom).astype(piece.dtype)
    owner = lax.rem(me[0] + 2, results.shape[0])
    copy = pltpu.make_async_copy(piece, results.at[owner], semaphores.at[3])
    copy.start()
    copy.wait()


VMEM = pl.BlockSpec(memory_space=pltpu.VMEM)
HBM = pl.BlockSpec(memory_space=pltpu.HBM)
SMEM = pl.BlockSpec(memory_space=pltpu.SMEM)


def shaped(shape, dtype=jnp.bfloat16):
    return jax.ShapeDtypeStruct(shape, dtype)


def slots_for(arrays):
    return [pltpu.VMEM(a.shape, a.dtype) for a in arrays]


def expert(rows, norm_gain, gate, up, down, gate_up_ring, down_ring, me):
    parts, count, width = rows.shape
    units = gate.shape[1]
    me = me.reshape(1)
    near, far = gate_up_ring
    near_down, far_down = down_ring
    given = [rows, gate, up, *near, *far, down, *near_down]
    whole = shaped((count, parts * units))
    hidden, results = pl.pallas_call(
        main_part,
        out_shape=(whole, shaped((parts, count, width))),
        in_specs=[SMEM, VMEM] + [HBM] * len(given),
        out_specs=(HBM, HBM),
        scratch_shapes=slots_for(given)
        + slots_for([shaped((count, parts * width)), whole, shaped((3, count, width))])
        + [pltpu.SemaphoreType.DMA((len(given),)), pltpu.SemaphoreType.DMA((4,))],
        name="main_part",
    )(me, norm_gain.reshape(parts, width), *given)
    given = [hidden, *far_down]
    return pl.pallas_call(
        last_part,
        out_shape=shaped((parts, count, width)),
        in_specs=[SMEM] + [HBM] * 4,
        out_specs=HBM,
        input_output_aliases={4: 0},
        scratch_shapes=slots_for(given)
        + slots_for([shaped((count, width))])
        + [pltpu.SemaphoreType.DMA((4,))],
        name="last_part",
    )(me, *given, results)


def layer(
    tokens,
    group_choice,
    expert_choice,
    group_weight,
    expert_weight,
    norm_gain,
    w_gate,
    w_up,
    w_down,
):
    tok_rows, piece_width = tokens.shape
    groups = lax.axis_size("g")
    members = lax.axis_size("m")
    tp_count = lax.axis_size("tp")
    me = lax.axis_index("tp")
    per_group = tok_rows // groups
    mean_load = 2 * tok_rows // (groups * members)
    capacity = mean_load + min(mean_load // 2, per_group - mean_load)
    chunks = piece_width // LANES
    depth = up_to(groups // tp_count * capacity, TILE)

    gate_up_ring = around(jnp.concatenate([w_gate[0], w_up[0]], 1), "tp")
    down_ring = around(w_down[0], "tp")

    blocks, rank = pl.pallas_call(
        depart,
        out_shape=(
            shaped((groups, chunks * per_group + TILE, LANES)),
            shaped((1, tok_rows), jnp.int32),
        ),
        in_specs=[VMEM] * 5,
        out_specs=(VMEM, VMEM),
        name="depart",
    )(group_choice, expert_choice.T, group_weight, expert_weight.T, tokens)
    rank = rank[0]
    landed = exchange(blocks, "g")

    facts_shape = (2, groups, LANES)
    buffer, targets, shares = pl.pallas_call(
        functools.partial(arrive, capacity),
        out_shape=(
            shaped((tp_count, members * depth, piece_width)),
            shaped(facts_shape, jnp.int32),
            shaped(facts_shape, jnp.float32),
        ),
        in_specs=[VMEM],
        out_specs=(VMEM, VMEM, VMEM),
        scratch_shapes=[pltpu.VMEM((groups, LANES, piece_width), jnp.bfloat16)],
        name="arrive",
    )(landed)
    rows = exchange(buffer.reshape(tp_count * members, depth, piece_width), BLOCK)
    rows = rows.reshape(tp_count, members * depth, piece_width)
    results = expert(
        rows, norm_gain, w_gate[0], w_up[0], w_down[0], gate_up_ring, down_ring, me
    )

    returned = exchange(results.reshape(tp_count * members, depth, piece_width), BLOCK)
    returned = returned.reshape(-1, piece_width)
    places = jnp.arange(returned.shape[0], dtype=jnp.int32)
    combined = jnp.zeros((tok_rows, piece_width), jnp.float32)
    for k in range(2):
        back = targets[k][:, :per_group].reshape(-1)
        share = shares[k][:, :per_group].reshape(-1)
        picker = (back[:, None] == places[None, :]).astype(jnp.bfloat16)
        combined = combined + share[:, None] * dot(picker, returned)
    combined = combined.astype(jnp.bfloat16)
    home = exchange(combined.reshape(groups, per_group, piece_width), "g")
    home = home.reshape(tok_rows, piece_width)
    here = lax.axis_index("g")
    seats = jnp.arange(per_group, dtype=jnp.int32)[None, :]
    stayed = (group_choice == here)[:, None] & (rank[:, None] == seats)
    own = lax.dynamic_slice_in_dim(combined, here * per_group, per_group, 0)
    kept = dot(stayed.astype(jnp.bfloat16), own)
    slot = jnp.where(group_choice == here, -1, group_choice * per_group + rank)
    unseating = slot[:, None] == jnp.arange(tok_rows, dtype=jnp.int32)[None, :]
    return (dot(unseating.astype(jnp.bfloat16), home) + kept).astype(jnp.bfloat16)


def solution(mesh):
    groups = mesh.shape["ep"] // GROUP_SIZE
    split = Mesh(
        mesh.devices.reshape(mesh.shape["grp"], groups, GROUP_SIZE, mesh.shape["tp"]),
        ("grp", "g", "m", "tp"),
    )
    placed = (
        P(GRP_EP, "tp"),
        P(GRP_EP),
        P(GRP_EP, None),
        P(GRP_EP),
        P(GRP_EP, None),
        P(),
        P(EP, None, "tp"),
        P(EP, None, "tp"),
        P(EP, None, "tp"),
    )
    return jax.shard_map(
        layer, mesh=split, in_specs=placed, out_specs=P(GRP_EP, "tp"), check_vma=False
    )
```

```python
import functools

import jax
import jax.numpy as jnp
from jax import lax
from jax.experimental import pallas as pl
from jax.experimental.pallas import tpu as pltpu
from jax.sharding import Mesh
from jax.sharding import PartitionSpec as P


GROUP_SIZE = 8
TILE = 8
LANES = 128
EP = ("g", "m")
GRP_EP = ("grp", "g", "m")
BLOCK = ("tp", "m")


def exchange(array, axis):
    return lax.all_to_all(array, axis, 0, 0, tiled=True)


def shifted(array, axis, by):
    length = lax.axis_size(axis)
    return lax.ppermute(array, axis, [(a, (a + by) % length) for a in range(length)])


def up_to(length, tile):
    return -(-length // tile) * tile


def around(array, axis):
    one = shifted(array, axis, 3)
    three = shifted(array, axis, 1)
    half = array.shape[0] // 2
    top = shifted(one[:half], axis, 3)
    bottom = shifted(three[half:], axis, 1)
    return [one, three], [top, bottom]


def dot(a, b):
    return jnp.dot(a, b, preferred_element_type=jnp.float32)


def fetch(sources, slots, semaphores):
    copies = [
        pltpu.make_async_copy(source, slot, semaphores.at[i])
        for i, (source, slot) in enumerate(zip(sources, slots, strict=True))
    ]
    for copy in copies:
        copy.start()
    return copies


def gated(both, units):
    gate, up = both[:, :units], both[:, units:]
    return (gate / (1.0 + jnp.exp(-gate)) * up).astype(jnp.bfloat16)


def iota(shape, dim):
    return lax.broadcasted_iota(jnp.int32, shape, dim)


def ones(condition):
    return jnp.where(condition, 1.0, 0.0).astype(jnp.bfloat16)


def depart(group, choice, group_share, expert_share, tokens, gate, up, *refs):
    blocks, ranks, joined, semaphores = refs
    units = gate.shape[1]
    sides = joined.at[:, pl.ds(0, units)], joined.at[:, pl.ds(units, units)]
    joining = fetch((gate, up), sides, semaphores)
    groups, _, lanes = blocks.shape
    count, width = tokens.shape
    chunks, per_group = width // lanes, count // groups
    group = group[...].reshape(1, count)
    member = group == iota((groups, count), 0)
    earlier = dot(ones(member), ones(iota((count, count), 0) < iota((count, count), 1)))
    rank = jnp.sum(jnp.where(member, earlier, 0.0), 0, keepdims=True).astype(jnp.int32)
    ranks[...] = rank
    seating = ones(iota((count, count), 0) == group * per_group + rank)
    seated = dot(seating, tokens[...]).astype(jnp.bfloat16)
    mixing = group_share[...].reshape(1, count) * expert_share[...]
    mixing = mixing / jnp.sum(expert_share[...], 0, keepdims=True)
    coarse = mixing.astype(jnp.bfloat16).astype(jnp.float32)
    fine = mixing - coarse
    choice = choice[...].astype(jnp.float32)
    facts = jnp.zeros((TILE, count), jnp.float32)
    for i, pair in enumerate((choice, coarse, fine)):
        for k in range(2):
            facts = jnp.where(iota((TILE, count), 0) == 2 * i + k, pair[k : k + 1], facts)
    spoken = [jnp.where(group == g, facts, 0.0) for g in range(groups)]
    spoken = jnp.concatenate(spoken, 0).astype(jnp.bfloat16)
    columns = ones(iota((lanes, count), 0) == rank)
    told = lax.dot_general(
        spoken, columns, (((1,), (1,)), ((), ())), preferred_element_type=jnp.float32
    ).astype(jnp.bfloat16)
    for g in range(groups):
        for c in range(chunks):
            piece = seated[g * per_group : (g + 1) * per_group, c * lanes : (c + 1) * lanes]
            blocks[g, c * per_group : (c + 1) * per_group, :] = piece
        blocks[g, chunks * per_group :, :] = told[g * TILE : (g + 1) * TILE]
    for copy in joining:
        copy.wait()


def arrive(capacity, landed, buffer, places, shares, seats):
    groups, lines, lanes = landed.shape
    parts, count, width = buffer.shape
    chunks = width // lanes
    per_group = (lines - TILE) // chunks
    members = GROUP_SIZE
    depth = count // members
    sources = groups // parts
    told = landed[:, chunks * per_group :, :].astype(jnp.float32)
    told = told.reshape(groups * TILE, lanes).astype(jnp.bfloat16)
    wanted = (6 * groups, groups * TILE)
    row = iota(wanted, 0)
    pick = iota(wanted, 1) == lax.rem(row, groups) * TILE + lax.div(row, groups)
    heard = dot(ones(pick), told)
    facts = [heard[i * groups : (i + 1) * groups] for i in range(6)]
    choices = [fact.astype(jnp.int32) for fact in facts[:2]]
    inside = iota((groups, lanes), 1) < per_group
    named = []
    for e in range(members):
        hit = (choices[0] == e) | (choices[1] == e)
        named.append(jnp.where(hit & inside, 1.0, 0.0))
    named = jnp.concatenate(named, 0).astype(jnp.bfloat16)
    earlier = dot(named, ones(iota((lanes, lanes), 0) < iota((lanes, lanes), 1)))
    source = iota((groups, lanes), 0)
    local = []
    for k in range(2):
        seat = jnp.zeros((groups, lanes), jnp.float32)
        for e in range(members):
            seat = jnp.where(choices[k] == e, earlier[e * groups : (e + 1) * groups], seat)
        place = choices[k] * depth + lax.rem(source, sources) * capacity + seat.astype(jnp.int32)
        local.append(jnp.where(inside, place, -1))
        places[k] = jnp.where(inside, lax.div(source, sources) * count + place, -1)
        shares[k] = facts[2 + k] + facts[4 + k]
    for g in range(groups):
        seats[g, per_group:, :] = jnp.zeros((lanes - per_group, width), jnp.bfloat16)
        for c in range(chunks):
            piece = landed[g, c * per_group : (c + 1) * per_group, :]
            seats[g, :per_group, c * lanes : (c + 1) * lanes] = piece
    rows = iota((count, lanes), 0)
    for p in range(parts):
        spread = []
        for g in range(p * sources, (p + 1) * sources):
            hit = (rows == local[0][g : g + 1]) | (rows == local[1][g : g + 1])
            spread.append(ones(hit))
        spread = jnp.concatenate(spread, 1)
        held = seats[p * sources : (p + 1) * sources].reshape(sources * lanes, width)
        buffer[p] = dot(spread, held).astype(jnp.bfloat16)


def gated(gate, up):
    return (gate / (1.0 + jnp.exp(-gate)) * up).astype(jnp.bfloat16)


def place(hidden, me, offset, parts, piece):
    units = piece.shape[1]
    at = pl.multiple_of(lax.rem(me[0] + offset, parts) * units, units)
    hidden[:, pl.ds(at, units)] = piece


def by_halves(whole, top, bottom):
    half = top.shape[0]
    return dot(whole[:, :half], top[...]) + dot(whole[:, half:], bottom[...])


def main_part(me, gains, *refs):
    given, (hidden_out, results), (rows, *slots) = refs[:10], refs[10:12], refs[12:22]
    normed, hidden, pieces, semaphores, leaving = refs[22:]
    gate, up, one, three, top, bottom, *down = slots
    arrived, *copies = fetch(given, (rows, *slots), semaphores)
    parts, _, width = rows.shape
    units = gate.shape[1]
    total = None
    arrived.wait()
    for t in range(parts):
        values = rows[t].astype(jnp.float32)
        squares = jnp.sum(values * values, -1, keepdims=True)
        total = squares if total is None else total + squares
    inv_rms = lax.rsqrt(total / (parts * width) + 1e-06)
    for t in range(parts):
        scaled = rows[t].astype(jnp.float32) * inv_rms * gains[t][None, :]
        normed[:, t * width : (t + 1) * width] = scaled.astype(jnp.bfloat16)
    copies[0].wait()
    copies[1].wait()
    piece = gated(dot(normed[...], gate[...]), dot(normed[...], up[...]))
    place(hidden, me, 0, parts, piece)
    for copy, slot, offset in zip(copies[2:4], (one, three), (1, 3), strict=True):
        copy.wait()
        both = dot(normed[...], slot[...])
        place(hidden, me, offset, parts, gated(both[:, :units], both[:, units:]))
    copies[4].wait()
    copies[5].wait()
    both = by_halves(normed, top, bottom)
    place(hidden, me, 2, parts, gated(both[:, :units], both[:, units:]))
    out = [pltpu.make_async_copy(hidden, hidden_out, leaving.at[3])]
    out[0].start()
    for i, offset in enumerate((0, 1, 3)):
        copies[6 + i].wait()
        pieces[i] = dot(hidden[...], down[i][...]).astype(pieces.dtype)
        owner = lax.rem(me[0] + offset, parts)
        out.append(pltpu.make_async_copy(pieces.at[i], results.at[owner], leaving.at[i]))
        out[-1].start()
    for copy in out:
        copy.wait()


def last_part(me, *refs):
    given, results, slots, piece, semaphores = refs[:3], refs[4], refs[5:8], refs[8], refs[9]
    for copy in fetch(given, slots, semaphores):
        copy.wait()
    hidden, top, bottom = slots
    piece[...] = by_halves(hidden, top, bottom).astype(piece.dtype)
    owner = lax.rem(me[0] + 2, results.shape[0])
    copy = pltpu.make_async_copy(piece, results.at[owner], semaphores.at[3])
    copy.start()
    copy.wait()


VMEM = pl.BlockSpec(memory_space=pltpu.VMEM)
HBM = pl.BlockSpec(memory_space=pltpu.HBM)
SMEM = pl.BlockSpec(memory_space=pltpu.SMEM)


def shaped(shape, dtype=jnp.bfloat16):
    return jax.ShapeDtypeStruct(shape, dtype)


def slots_for(arrays):
    return [pltpu.VMEM(a.shape, a.dtype) for a in arrays]


def expert(rows, norm_gain, gate, up, down, gate_up_ring, down_ring, me):
    parts, count, width = rows.shape
    units = gate.shape[1]
    me = me.reshape(1)
    near, far = gate_up_ring
    near_down, far_down = down_ring
    given = [rows, gate, up, *near, *far, down, *near_down]
    whole = shaped((count, parts * units))
    hidden, results = pl.pallas_call(
        main_part,
        out_shape=(whole, shaped((parts, count, width))),
        in_specs=[SMEM, VMEM] + [HBM] * len(given),
        out_specs=(HBM, HBM),
        scratch_shapes=slots_for(given)
        + slots_for([shaped((count, parts * width)), whole, shaped((3, count, width))])
        + [pltpu.SemaphoreType.DMA((len(given),)), pltpu.SemaphoreType.DMA((4,))],
        name="main_part",
    )(me, norm_gain.reshape(parts, width), *given)
    given = [hidden, *far_down]
    return pl.pallas_call(
        last_part,
        out_shape=shaped((parts, count, width)),
        in_specs=[SMEM] + [HBM] * 4,
        out_specs=HBM,
        input_output_aliases={4: 0},
        scratch_shapes=slots_for(given)
        + slots_for([shaped((count, width))])
        + [pltpu.SemaphoreType.DMA((4,))],
        name="last_part",
    )(me, *given, results)


def layer(
    tokens,
    group_choice,
    expert_choice,
    group_weight,
    expert_weight,
    norm_gain,
    w_gate,
    w_up,
    w_down,
):
    tok_rows, piece_width = tokens.shape
    groups = lax.axis_size("g")
    members = lax.axis_size("m")
    tp_count = lax.axis_size("tp")
    me = lax.axis_index("tp")
    per_group = tok_rows // groups
    mean_load = 2 * tok_rows // (groups * members)
    capacity = mean_load + min(mean_load // 2, per_group - mean_load)
    chunks = piece_width // LANES
    depth = up_to(groups // tp_count * capacity, TILE)

    gate, up, down = w_gate[0], w_up[0], w_down[0]
    blocks, rank, joined = pl.pallas_call(
        depart,
        out_shape=(
            shaped((groups, chunks * per_group + TILE, LANES)),
            shaped((1, tok_rows), jnp.int32),
            shaped((gate.shape[0], 2 * gate.shape[1])),
        ),
        in_specs=[VMEM] * 5 + [HBM] * 2,
        out_specs=(VMEM, VMEM, HBM),
        scratch_shapes=[pltpu.SemaphoreType.DMA((2,))],
        name="depart",
    )(group_choice, expert_choice.T, group_weight, expert_weight.T, tokens, gate, up)
    gate_up_ring = around(joined, "tp")
    down_ring = around(down, "tp")
    rank = rank[0]
    landed = exchange(blocks, "g")

    facts_shape = (2, groups, LANES)
    buffer, targets, shares = pl.pallas_call(
        functools.partial(arrive, capacity),
        out_shape=(
            shaped((tp_count, members * depth, piece_width)),
            shaped(facts_shape, jnp.int32),
            shaped(facts_shape, jnp.float32),
        ),
        in_specs=[VMEM],
        out_specs=(VMEM, VMEM, VMEM),
        scratch_shapes=[pltpu.VMEM((groups, LANES, piece_width), jnp.bfloat16)],
        name="arrive",
    )(landed)
    rows = exchange(buffer.reshape(tp_count * members, depth, piece_width), BLOCK)
    rows = rows.reshape(tp_count, members * depth, piece_width)
    results = expert(rows, norm_gain, gate, up, down, gate_up_ring, down_ring, me)

    returned = exchange(results.reshape(tp_count * members, depth, piece_width), BLOCK)
    returned = returned.reshape(-1, piece_width)
    places = jnp.arange(returned.shape[0], dtype=jnp.int32)
    combined = jnp.zeros((tok_rows, piece_width), jnp.float32)
    for k in range(2):
        back = targets[k][:, :per_group].reshape(-1)
        share = shares[k][:, :per_group].reshape(-1)
        picker = (back[:, None] == places[None, :]).astype(jnp.bfloat16)
        combined = combined + share[:, None] * dot(picker, returned)
    combined = combined.astype(jnp.bfloat16)
    home = exchange(combined.reshape(groups, per_group, piece_width), "g")
    home = home.reshape(tok_rows, piece_width)
    here = lax.axis_index("g")
    seats = jnp.arange(per_group, dtype=jnp.int32)[None, :]
    stayed = (group_choice == here)[:, None] & (rank[:, None] == seats)
    own = lax.dynamic_slice_in_dim(combined, here * per_group, per_group, 0)
    kept = dot(stayed.astype(jnp.bfloat16), own)
    slot = jnp.where(group_choice == here, -1, group_choice * per_group + rank)
    unseating = slot[:, None] == jnp.arange(tok_rows, dtype=jnp.int32)[None, :]
    return (dot(unseating.astype(jnp.bfloat16), home) + kept).astype(jnp.bfloat16)


def solution(mesh):
    groups = mesh.shape["ep"] // GROUP_SIZE
    split = Mesh(
        mesh.devices.reshape(mesh.shape["grp"], groups, GROUP_SIZE, mesh.shape["tp"]),
        ("grp", "g", "m", "tp"),
    )
    placed = (
        P(GRP_EP, "tp"),
        P(GRP_EP),
        P(GRP_EP, None),
        P(GRP_EP),
        P(GRP_EP, None),
        P(),
        P(EP, None, "tp"),
        P(EP, None, "tp"),
        P(EP, None, "tp"),
    )
    return jax.shard_map(
        layer, mesh=split, in_specs=placed, out_specs=P(GRP_EP, "tp"), check_vma=False
    )
```

```python
import functools

import jax
import jax.numpy as jnp
from jax import lax
from jax.experimental import pallas as pl
from jax.experimental.pallas import tpu as pltpu
from jax.sharding import Mesh
from jax.sharding import PartitionSpec as P


GROUP_SIZE = 8
TILE = 8
LANES = 128
EP = ("g", "m")
GRP_EP = ("grp", "g", "m")
BLOCK = ("tp", "m")


def exchange(array, axis):
    return lax.all_to_all(array, axis, 0, 0, tiled=True)


def shifted(array, axis, by):
    length = lax.axis_size(axis)
    return lax.ppermute(array, axis, [(a, (a + by) % length) for a in range(length)])


def up_to(length, tile):
    return -(-length // tile) * tile


def around(array, axis):
    one = shifted(array, axis, 3)
    three = shifted(array, axis, 1)
    half = array.shape[0] // 2
    top = shifted(one[:half], axis, 3)
    bottom = shifted(three[half:], axis, 1)
    return [one, three], [top, bottom]


def dot(a, b):
    return jnp.dot(a, b, preferred_element_type=jnp.float32)


def fetch(sources, slots, semaphores):
    copies = [
        pltpu.make_async_copy(source, slot, semaphores.at[i])
        for i, (source, slot) in enumerate(zip(sources, slots, strict=True))
    ]
    for copy in copies:
        copy.start()
    return copies


def gated(both, units):
    gate, up = both[:, :units], both[:, units:]
    return (gate / (1.0 + jnp.exp(-gate)) * up).astype(jnp.bfloat16)


def iota(shape, dim):
    return lax.broadcasted_iota(jnp.int32, shape, dim)


def ones(condition):
    return jnp.where(condition, 1.0, 0.0).astype(jnp.bfloat16)


def depart(group, choice, group_share, expert_share, tokens, gate, up, *refs):
    blocks, ranks, joined, held, semaphores = refs
    units = gate.shape[1]
    sides = held.at[:, pl.ds(0, units)], held.at[:, pl.ds(units, units)]
    joining = fetch((gate, up), sides, semaphores)
    groups, _, lanes = blocks.shape
    count, width = tokens.shape
    chunks, per_group = width // lanes, count // groups
    group = group[...].reshape(1, count)
    member = group == iota((groups, count), 0)
    earlier = dot(ones(member), ones(iota((count, count), 0) < iota((count, count), 1)))
    rank = jnp.sum(jnp.where(member, earlier, 0.0), 0, keepdims=True).astype(jnp.int32)
    ranks[...] = rank
    seating = ones(iota((count, count), 0) == group * per_group + rank)
    for copy in joining:
        copy.wait()
    leaving = pltpu.make_async_copy(held, joined, semaphores.at[2])
    leaving.start()
    seated = dot(seating, tokens[...]).astype(jnp.bfloat16)
    mixing = group_share[...].reshape(1, count) * expert_share[...]
    mixing = mixing / jnp.sum(expert_share[...], 0, keepdims=True)
    coarse = mixing.astype(jnp.bfloat16).astype(jnp.float32)
    fine = mixing - coarse
    choice = choice[...].astype(jnp.float32)
    facts = jnp.zeros((TILE, count), jnp.float32)
    for i, pair in enumerate((choice, coarse, fine)):
        for k in range(2):
            facts = jnp.where(iota((TILE, count), 0) == 2 * i + k, pair[k : k + 1], facts)
    spoken = [jnp.where(group == g, facts, 0.0) for g in range(groups)]
    spoken = jnp.concatenate(spoken, 0).astype(jnp.bfloat16)
    columns = ones(iota((lanes, count), 0) == rank)
    told = lax.dot_general(
        spoken, columns, (((1,), (1,)), ((), ())), preferred_element_type=jnp.float32
    ).astype(jnp.bfloat16)
    for g in range(groups):
        for c in range(chunks):
            piece = seated[g * per_group : (g + 1) * per_group, c * lanes : (c + 1) * lanes]
            blocks[g, c * per_group : (c + 1) * per_group, :] = piece
        blocks[g, chunks * per_group :, :] = told[g * TILE : (g + 1) * TILE]
    leaving.wait()


def arrive(capacity, landed, buffer, places, shares, seats):
    groups, lines, lanes = landed.shape
    parts, count, width = buffer.shape
    chunks = width // lanes
    per_group = (lines - TILE) // chunks
    members = GROUP_SIZE
    depth = count // members
    sources = groups // parts
    told = landed[:, chunks * per_group :, :].astype(jnp.float32)
    told = told.reshape(groups * TILE, lanes).astype(jnp.bfloat16)
    wanted = (6 * groups, groups * TILE)
    row = iota(wanted, 0)
    pick = iota(wanted, 1) == lax.rem(row, groups) * TILE + lax.div(row, groups)
    heard = dot(ones(pick), told)
    facts = [heard[i * groups : (i + 1) * groups] for i in range(6)]
    choices = [fact.astype(jnp.int32) for fact in facts[:2]]
    inside = iota((groups, lanes), 1) < per_group
    named = []
    for e in range(members):
        hit = (choices[0] == e) | (choices[1] == e)
        named.append(jnp.where(hit & inside, 1.0, 0.0))
    named = jnp.concatenate(named, 0).astype(jnp.bfloat16)
    earlier = dot(named, ones(iota((lanes, lanes), 0) < iota((lanes, lanes), 1)))
    source = iota((groups, lanes), 0)
    local = []
    for k in range(2):
        seat = jnp.zeros((groups, lanes), jnp.float32)
        for e in range(members):
            seat = jnp.where(choices[k] == e, earlier[e * groups : (e + 1) * groups], seat)
        place = choices[k] * depth + lax.rem(source, sources) * capacity + seat.astype(jnp.int32)
        local.append(jnp.where(inside, place, -1))
        places[k] = jnp.where(inside, lax.div(source, sources) * count + place, -1)
        shares[k] = facts[2 + k] + facts[4 + k]
    for g in range(groups):
        seats[g, per_group:, :] = jnp.zeros((lanes - per_group, width), jnp.bfloat16)
        for c in range(chunks):
            piece = landed[g, c * per_group : (c + 1) * per_group, :]
            seats[g, :per_group, c * lanes : (c + 1) * lanes] = piece
    rows = iota((count, lanes), 0)
    for p in range(parts):
        spread = []
        for g in range(p * sources, (p + 1) * sources):
            hit = (rows == local[0][g : g + 1]) | (rows == local[1][g : g + 1])
            spread.append(ones(hit))
        spread = jnp.concatenate(spread, 1)
        held = seats[p * sources : (p + 1) * sources].reshape(sources * lanes, width)
        buffer[p] = dot(spread, held).astype(jnp.bfloat16)


def gated(gate, up):
    return (gate / (1.0 + jnp.exp(-gate)) * up).astype(jnp.bfloat16)


def place(hidden, me, offset, parts, piece):
    units = piece.shape[1]
    at = pl.multiple_of(lax.rem(me[0] + offset, parts) * units, units)
    hidden[:, pl.ds(at, units)] = piece


def by_halves(whole, top, bottom):
    half = top.shape[0]
    return dot(whole[:, :half], top[...]) + dot(whole[:, half:], bottom[...])


def main_part(me, gains, *refs):
    given, (hidden_out, results), (rows, *slots) = refs[:10], refs[10:12], refs[12:22]
    normed, hidden, pieces, semaphores, leaving = refs[22:]
    gate, up, one, three, top, bottom, *down = slots
    arrived, *copies = fetch(given, (rows, *slots), semaphores)
    parts, _, width = rows.shape
    units = gate.shape[1]
    total = None
    arrived.wait()
    for t in range(parts):
        values = rows[t].astype(jnp.float32)
        squares = jnp.sum(values * values, -1, keepdims=True)
        total = squares if total is None else total + squares
    inv_rms = lax.rsqrt(total / (parts * width) + 1e-06)
    for t in range(parts):
        scaled = rows[t].astype(jnp.float32) * inv_rms * gains[t][None, :]
        normed[:, t * width : (t + 1) * width] = scaled.astype(jnp.bfloat16)
    copies[0].wait()
    copies[1].wait()
    piece = gated(dot(normed[...], gate[...]), dot(normed[...], up[...]))
    place(hidden, me, 0, parts, piece)
    for copy, slot, offset in zip(copies[2:4], (one, three), (1, 3), strict=True):
        copy.wait()
        both = dot(normed[...], slot[...])
        place(hidden, me, offset, parts, gated(both[:, :units], both[:, units:]))
    copies[4].wait()
    copies[5].wait()
    both = by_halves(normed, top, bottom)
    place(hidden, me, 2, parts, gated(both[:, :units], both[:, units:]))
    out = [pltpu.make_async_copy(hidden, hidden_out, leaving.at[3])]
    out[0].start()
    for i, offset in enumerate((0, 1, 3)):
        copies[6 + i].wait()
        pieces[i] = dot(hidden[...], down[i][...]).astype(pieces.dtype)
        owner = lax.rem(me[0] + offset, parts)
        out.append(pltpu.make_async_copy(pieces.at[i], results.at[owner], leaving.at[i]))
        out[-1].start()
    for copy in out:
        copy.wait()


def last_part(me, *refs):
    given, results, slots, piece, semaphores = refs[:3], refs[4], refs[5:8], refs[8], refs[9]
    for copy in fetch(given, slots, semaphores):
        copy.wait()
    hidden, top, bottom = slots
    piece[...] = by_halves(hidden, top, bottom).astype(piece.dtype)
    owner = lax.rem(me[0] + 2, results.shape[0])
    copy = pltpu.make_async_copy(piece, results.at[owner], semaphores.at[3])
    copy.start()
    copy.wait()


VMEM = pl.BlockSpec(memory_space=pltpu.VMEM)
HBM = pl.BlockSpec(memory_space=pltpu.HBM)
SMEM = pl.BlockSpec(memory_space=pltpu.SMEM)


def shaped(shape, dtype=jnp.bfloat16):
    return jax.ShapeDtypeStruct(shape, dtype)


def slots_for(arrays):
    return [pltpu.VMEM(a.shape, a.dtype) for a in arrays]


def expert(rows, norm_gain, gate, up, down, gate_up_ring, down_ring, me):
    parts, count, width = rows.shape
    units = gate.shape[1]
    me = me.reshape(1)
    near, far = gate_up_ring
    near_down, far_down = down_ring
    given = [rows, gate, up, *near, *far, down, *near_down]
    whole = shaped((count, parts * units))
    hidden, results = pl.pallas_call(
        main_part,
        out_shape=(whole, shaped((parts, count, width))),
        in_specs=[SMEM, VMEM] + [HBM] * len(given),
        out_specs=(HBM, HBM),
        scratch_shapes=slots_for(given)
        + slots_for([shaped((count, parts * width)), whole, shaped((3, count, width))])
        + [pltpu.SemaphoreType.DMA((len(given),)), pltpu.SemaphoreType.DMA((4,))],
        name="main_part",
    )(me, norm_gain.reshape(parts, width), *given)
    given = [hidden, *far_down]
    return pl.pallas_call(
        last_part,
        out_shape=shaped((parts, count, width)),
        in_specs=[SMEM] + [HBM] * 4,
        out_specs=HBM,
        input_output_aliases={4: 0},
        scratch_shapes=slots_for(given)
        + slots_for([shaped((count, width))])
        + [pltpu.SemaphoreType.DMA((4,))],
        name="last_part",
    )(me, *given, results)


def layer(
    tokens,
    group_choice,
    expert_choice,
    group_weight,
    expert_weight,
    norm_gain,
    w_gate,
    w_up,
    w_down,
):
    tok_rows, piece_width = tokens.shape
    groups = lax.axis_size("g")
    members = lax.axis_size("m")
    tp_count = lax.axis_size("tp")
    me = lax.axis_index("tp")
    per_group = tok_rows // groups
    mean_load = 2 * tok_rows // (groups * members)
    capacity = mean_load + min(mean_load // 2, per_group - mean_load)
    chunks = piece_width // LANES
    depth = up_to(groups // tp_count * capacity, TILE)

    gate, up, down = w_gate[0], w_up[0], w_down[0]
    blocks, rank, joined = pl.pallas_call(
        depart,
        out_shape=(
            shaped((groups, chunks * per_group + TILE, LANES)),
            shaped((1, tok_rows), jnp.int32),
            shaped((gate.shape[0], 2 * gate.shape[1])),
        ),
        in_specs=[VMEM] * 5 + [HBM] * 2,
        out_specs=(VMEM, VMEM, HBM),
        scratch_shapes=[
            pltpu.VMEM((gate.shape[0], 2 * gate.shape[1]), jnp.bfloat16),
            pltpu.SemaphoreType.DMA((3,)),
        ],
        name="depart",
    )(group_choice, expert_choice.T, group_weight, expert_weight.T, tokens, gate, up)
    gate_up_ring = around(joined, "tp")
    down_ring = around(down, "tp")
    rank = rank[0]
    landed = exchange(blocks, "g")

    facts_shape = (2, groups, LANES)
    buffer, targets, shares = pl.pallas_call(
        functools.partial(arrive, capacity),
        out_shape=(
            shaped((tp_count, members * depth, piece_width)),
            shaped(facts_shape, jnp.int32),
            shaped(facts_shape, jnp.float32),
        ),
        in_specs=[VMEM],
        out_specs=(VMEM, VMEM, VMEM),
        scratch_shapes=[pltpu.VMEM((groups, LANES, piece_width), jnp.bfloat16)],
        name="arrive",
    )(landed)
    rows = exchange(buffer.reshape(tp_count * members, depth, piece_width), BLOCK)
    rows = rows.reshape(tp_count, members * depth, piece_width)
    results = expert(rows, norm_gain, gate, up, down, gate_up_ring, down_ring, me)

    returned = exchange(results.reshape(tp_count * members, depth, piece_width), BLOCK)
    returned = returned.reshape(-1, piece_width)
    places = jnp.arange(returned.shape[0], dtype=jnp.int32)
    combined = jnp.zeros((tok_rows, piece_width), jnp.float32)
    for k in range(2):
        back = targets[k][:, :per_group].reshape(-1)
        share = shares[k][:, :per_group].reshape(-1)
        picker = (back[:, None] == places[None, :]).astype(jnp.bfloat16)
        combined = combined + share[:, None] * dot(picker, returned)
    combined = combined.astype(jnp.bfloat16)
    home = exchange(combined.reshape(groups, per_group, piece_width), "g")
    home = home.reshape(tok_rows, piece_width)
    here = lax.axis_index("g")
    seats = jnp.arange(per_group, dtype=jnp.int32)[None, :]
    stayed = (group_choice == here)[:, None] & (rank[:, None] == seats)
    own = lax.dynamic_slice_in_dim(combined, here * per_group, per_group, 0)
    kept = dot(stayed.astype(jnp.bfloat16), own)
    slot = jnp.where(group_choice == here, -1, group_choice * per_group + rank)
    unseating = slot[:, None] == jnp.arange(tok_rows, dtype=jnp.int32)[None, :]
    return (dot(unseating.astype(jnp.bfloat16), home) + kept).astype(jnp.bfloat16)


def solution(mesh):
    groups = mesh.shape["ep"] // GROUP_SIZE
    split = Mesh(
        mesh.devices.reshape(mesh.shape["grp"], groups, GROUP_SIZE, mesh.shape["tp"]),
        ("grp", "g", "m", "tp"),
    )
    placed = (
        P(GRP_EP, "tp"),
        P(GRP_EP),
        P(GRP_EP, None),
        P(GRP_EP),
        P(GRP_EP, None),
        P(),
        P(EP, None, "tp"),
        P(EP, None, "tp"),
        P(EP, None, "tp"),
    )
    return jax.shard_map(
        layer, mesh=split, in_specs=placed, out_specs=P(GRP_EP, "tp"), check_vma=False
    )
```

```python
import functools

import jax
import jax.numpy as jnp
from jax import lax
from jax.experimental import pallas as pl
from jax.experimental.pallas import tpu as pltpu
from jax.sharding import Mesh
from jax.sharding import PartitionSpec as P


GROUP_SIZE = 8
TILE = 8
LANES = 128
EP = ("g", "m")
GRP_EP = ("grp", "g", "m")
BLOCK = ("tp", "m")


def exchange(array, axis):
    return lax.all_to_all(array, axis, 0, 0, tiled=True)


def shifted(array, axis, by):
    length = lax.axis_size(axis)
    return lax.ppermute(array, axis, [(a, (a + by) % length) for a in range(length)])


def up_to(length, tile):
    return -(-length // tile) * tile


def around(array, axis):
    one = shifted(array, axis, 3)
    three = shifted(array, axis, 1)
    half = array.shape[0] // 2
    top = shifted(one[:half], axis, 3)
    bottom = shifted(three[half:], axis, 1)
    return [one, three], [top, bottom]


def dot(a, b):
    return jnp.dot(a, b, preferred_element_type=jnp.float32)


def fetch(sources, slots, semaphores):
    copies = [
        pltpu.make_async_copy(source, slot, semaphores.at[i])
        for i, (source, slot) in enumerate(zip(sources, slots, strict=True))
    ]
    for copy in copies:
        copy.start()
    return copies


def gated(both, units):
    gate, up = both[:, :units], both[:, units:]
    return (gate / (1.0 + jnp.exp(-gate)) * up).astype(jnp.bfloat16)


def iota(shape, dim):
    return lax.broadcasted_iota(jnp.int32, shape, dim)


def ones(condition):
    return jnp.where(condition, 1.0, 0.0).astype(jnp.bfloat16)


def depart(group, choice, group_share, expert_share, tokens, blocks, ranks):
    groups, _, lanes = blocks.shape
    count, width = tokens.shape
    chunks, per_group = width // lanes, count // groups
    group = group[...].reshape(1, count)
    member = group == iota((groups, count), 0)
    earlier = dot(ones(member), ones(iota((count, count), 0) < iota((count, count), 1)))
    rank = jnp.sum(jnp.where(member, earlier, 0.0), 0, keepdims=True).astype(jnp.int32)
    ranks[...] = rank
    seating = ones(iota((count, count), 0) == group * per_group + rank)
    seated = dot(seating, tokens[...]).astype(jnp.bfloat16)
    mixing = group_share[...].reshape(1, count) * expert_share[...]
    mixing = mixing / jnp.sum(expert_share[...], 0, keepdims=True)
    coarse = mixing.astype(jnp.bfloat16).astype(jnp.float32)
    fine = mixing - coarse
    choice = choice[...].astype(jnp.float32)
    facts = jnp.zeros((TILE, count), jnp.float32)
    for i, pair in enumerate((choice, coarse, fine)):
        for k in range(2):
            facts = jnp.where(iota((TILE, count), 0) == 2 * i + k, pair[k : k + 1], facts)
    spoken = [jnp.where(group == g, facts, 0.0) for g in range(groups)]
    spoken = jnp.concatenate(spoken, 0).astype(jnp.bfloat16)
    columns = ones(iota((lanes, count), 0) == rank)
    told = lax.dot_general(
        spoken, columns, (((1,), (1,)), ((), ())), preferred_element_type=jnp.float32
    ).astype(jnp.bfloat16)
    for g in range(groups):
        for c in range(chunks):
            piece = seated[g * per_group : (g + 1) * per_group, c * lanes : (c + 1) * lanes]
            blocks[g, c * per_group : (c + 1) * per_group, :] = piece
        blocks[g, chunks * per_group :, :] = told[g * TILE : (g + 1) * TILE]


def arrive(capacity, landed, buffer, places, shares, seats):
    groups, lines, lanes = landed.shape
    parts, count, width = buffer.shape
    chunks = width // lanes
    per_group = (lines - TILE) // chunks
    members = GROUP_SIZE
    depth = count // members
    sources = groups // parts
    told = landed[:, chunks * per_group :, :].astype(jnp.float32)
    told = told.reshape(groups * TILE, lanes).astype(jnp.bfloat16)
    wanted = (6 * groups, groups * TILE)
    row = iota(wanted, 0)
    pick = iota(wanted, 1) == lax.rem(row, groups) * TILE + lax.div(row, groups)
    heard = dot(ones(pick), told)
    facts = [heard[i * groups : (i + 1) * groups] for i in range(6)]
    choices = [fact.astype(jnp.int32) for fact in facts[:2]]
    inside = iota((groups, lanes), 1) < per_group
    named = []
    for e in range(members):
        hit = (choices[0] == e) | (choices[1] == e)
        named.append(jnp.where(hit & inside, 1.0, 0.0))
    named = jnp.concatenate(named, 0).astype(jnp.bfloat16)
    earlier = dot(named, ones(iota((lanes, lanes), 0) < iota((lanes, lanes), 1)))
    source = iota((groups, lanes), 0)
    local = []
    for k in range(2):
        seat = jnp.zeros((groups, lanes), jnp.float32)
        for e in range(members):
            seat = jnp.where(choices[k] == e, earlier[e * groups : (e + 1) * groups], seat)
        place = choices[k] * depth + lax.rem(source, sources) * capacity + seat.astype(jnp.int32)
        local.append(jnp.where(inside, place, -1))
        places[k] = jnp.where(inside, lax.div(source, sources) * count + place, -1)
        shares[k] = facts[2 + k] + facts[4 + k]
    for g in range(groups):
        seats[g, per_group:, :] = jnp.zeros((lanes - per_group, width), jnp.bfloat16)
        for c in range(chunks):
            piece = landed[g, c * per_group : (c + 1) * per_group, :]
            seats[g, :per_group, c * lanes : (c + 1) * lanes] = piece
    rows = iota((count, lanes), 0)
    for p in range(parts):
        spread = []
        for g in range(p * sources, (p + 1) * sources):
            hit = (rows == local[0][g : g + 1]) | (rows == local[1][g : g + 1])
            spread.append(ones(hit))
        spread = jnp.concatenate(spread, 1)
        held = seats[p * sources : (p + 1) * sources].reshape(sources * lanes, width)
        buffer[p] = dot(spread, held).astype(jnp.bfloat16)


def gated(gate, up):
    return (gate / (1.0 + jnp.exp(-gate)) * up).astype(jnp.bfloat16)


def place(hidden, me, offset, parts, piece):
    units = piece.shape[1]
    at = pl.multiple_of(lax.rem(me[0] + offset, parts) * units, units)
    hidden[:, pl.ds(at, units)] = piece


def by_halves(whole, top, bottom):
    half = top.shape[0]
    return dot(whole[:, :half], top[...]) + dot(whole[:, half:], bottom[...])


def main_part(me, gains, *refs):
    given, (hidden_out, results), (rows, *slots) = refs[:10], refs[10:12], refs[12:22]
    normed, hidden, pieces, semaphores, leaving = refs[22:]
    gate, up, one, three, top, bottom, *down = slots
    arrived, *copies = fetch(given[:3], (rows, *slots[:2]), semaphores)
    parts, _, width = rows.shape
    units = gate.shape[1]
    total = None
    arrived.wait()
    copies += fetch(given[3:], slots[2:], semaphores.at[pl.ds(3, len(given) - 3)])
    for t in range(parts):
        values = rows[t].astype(jnp.float32)
        squares = jnp.sum(values * values, -1, keepdims=True)
        total = squares if total is None else total + squares
    inv_rms = lax.rsqrt(total / (parts * width) + 1e-06)
    for t in range(parts):
        scaled = rows[t].astype(jnp.float32) * inv_rms * gains[t][None, :]
        normed[:, t * width : (t + 1) * width] = scaled.astype(jnp.bfloat16)
    copies[0].wait()
    copies[1].wait()
    piece = gated(dot(normed[...], gate[...]), dot(normed[...], up[...]))
    place(hidden, me, 0, parts, piece)
    for copy, slot, offset in zip(copies[2:4], (one, three), (1, 3), strict=True):
        copy.wait()
        both = dot(normed[...], slot[...])
        place(hidden, me, offset, parts, gated(both[:, :units], both[:, units:]))
    copies[4].wait()
    copies[5].wait()
    both = by_halves(normed, top, bottom)
    place(hidden, me, 2, parts, gated(both[:, :units], both[:, units:]))
    out = [pltpu.make_async_copy(hidden, hidden_out, leaving.at[3])]
    out[0].start()
    for i, offset in enumerate((0, 1, 3)):
        copies[6 + i].wait()
        pieces[i] = dot(hidden[...], down[i][...]).astype(pieces.dtype)
        owner = lax.rem(me[0] + offset, parts)
        out.append(pltpu.make_async_copy(pieces.at[i], results.at[owner], leaving.at[i]))
        out[-1].start()
    for copy in out:
        copy.wait()


def last_part(me, *refs):
    given, results, slots, piece, semaphores = refs[:3], refs[4], refs[5:8], refs[8], refs[9]
    for copy in fetch(given, slots, semaphores):
        copy.wait()
    hidden, top, bottom = slots
    piece[...] = by_halves(hidden, top, bottom).astype(piece.dtype)
    owner = lax.rem(me[0] + 2, results.shape[0])
    copy = pltpu.make_async_copy(piece, results.at[owner], semaphores.at[3])
    copy.start()
    copy.wait()


VMEM = pl.BlockSpec(memory_space=pltpu.VMEM)
HBM = pl.BlockSpec(memory_space=pltpu.HBM)
SMEM = pl.BlockSpec(memory_space=pltpu.SMEM)


def shaped(shape, dtype=jnp.bfloat16):
    return jax.ShapeDtypeStruct(shape, dtype)


def slots_for(arrays):
    return [pltpu.VMEM(a.shape, a.dtype) for a in arrays]


def expert(rows, norm_gain, gate, up, down, gate_up_ring, down_ring, me):
    parts, count, width = rows.shape
    units = gate.shape[1]
    me = me.reshape(1)
    near, far = gate_up_ring
    near_down, far_down = down_ring
    given = [rows, gate, up, *near, *far, down, *near_down]
    whole = shaped((count, parts * units))
    hidden, results = pl.pallas_call(
        main_part,
        out_shape=(whole, shaped((parts, count, width))),
        in_specs=[SMEM, VMEM] + [HBM] * len(given),
        out_specs=(HBM, HBM),
        scratch_shapes=slots_for(given)
        + slots_for([shaped((count, parts * width)), whole, shaped((3, count, width))])
        + [pltpu.SemaphoreType.DMA((len(given),)), pltpu.SemaphoreType.DMA((4,))],
        name="main_part",
    )(me, norm_gain.reshape(parts, width), *given)
    given = [hidden, *far_down]
    return pl.pallas_call(
        last_part,
        out_shape=shaped((parts, count, width)),
        in_specs=[SMEM] + [HBM] * 4,
        out_specs=HBM,
        input_output_aliases={4: 0},
        scratch_shapes=slots_for(given)
        + slots_for([shaped((count, width))])
        + [pltpu.SemaphoreType.DMA((4,))],
        name="last_part",
    )(me, *given, results)


def layer(
    tokens,
    group_choice,
    expert_choice,
    group_weight,
    expert_weight,
    norm_gain,
    w_gate,
    w_up,
    w_down,
):
    tok_rows, piece_width = tokens.shape
    groups = lax.axis_size("g")
    members = lax.axis_size("m")
    tp_count = lax.axis_size("tp")
    me = lax.axis_index("tp")
    per_group = tok_rows // groups
    mean_load = 2 * tok_rows // (groups * members)
    capacity = mean_load + min(mean_load // 2, per_group - mean_load)
    chunks = piece_width // LANES
    depth = up_to(groups // tp_count * capacity, TILE)

    gate_up_ring = around(jnp.concatenate([w_gate[0], w_up[0]], 1), "tp")
    down_ring = around(w_down[0], "tp")

    blocks, rank = pl.pallas_call(
        depart,
        out_shape=(
            shaped((groups, chunks * per_group + TILE, LANES)),
            shaped((1, tok_rows), jnp.int32),
        ),
        in_specs=[VMEM] * 5,
        out_specs=(VMEM, VMEM),
        name="depart",
    )(group_choice, expert_choice.T, group_weight, expert_weight.T, tokens)
    rank = rank[0]
    landed = exchange(blocks, "g")

    facts_shape = (2, groups, LANES)
    buffer, targets, shares = pl.pallas_call(
        functools.partial(arrive, capacity),
        out_shape=(
            shaped((tp_count, members * depth, piece_width)),
            shaped(facts_shape, jnp.int32),
            shaped(facts_shape, jnp.float32),
        ),
        in_specs=[VMEM],
        out_specs=(VMEM, VMEM, VMEM),
        scratch_shapes=[pltpu.VMEM((groups, LANES, piece_width), jnp.bfloat16)],
        name="arrive",
    )(landed)
    rows = exchange(buffer.reshape(tp_count * members, depth, piece_width), BLOCK)
    rows = rows.reshape(tp_count, members * depth, piece_width)
    results = expert(
        rows, norm_gain, w_gate[0], w_up[0], w_down[0], gate_up_ring, down_ring, me
    )

    places = jnp.arange(tp_count * members * depth, dtype=jnp.int32)
    targets, shares, results = lax.optimization_barrier((targets, shares, results))
    coarse = lax.reduce_precision(shares, 8, 7)
    mixers = []
    for share in (coarse, shares - coarse):
        weights = 0.0
        for k in range(2):
            back = targets[k][:, :per_group].reshape(-1)
            part = share[k][:, :per_group].reshape(-1)
            weights += jnp.where(back[:, None] == places[None, :], part[:, None], 0.0)
        mixers.append(weights.astype(jnp.bfloat16))
    mixers = lax.optimization_barrier(mixers)
    returned = exchange(results.reshape(tp_count * members, depth, piece_width), BLOCK)
    returned = returned.reshape(-1, piece_width)
    combined = sum(dot(weights, returned) for weights in mixers).astype(jnp.bfloat16)
    home = exchange(combined.reshape(groups, per_group, piece_width), "g")
    home = home.reshape(tok_rows, piece_width)
    here = lax.axis_index("g")
    seats = jnp.arange(per_group, dtype=jnp.int32)[None, :]
    stayed = (group_choice == here)[:, None] & (rank[:, None] == seats)
    own = lax.dynamic_slice_in_dim(combined, here * per_group, per_group, 0)
    kept = lax.optimization_barrier(dot(stayed.astype(jnp.bfloat16), own))
    slot = jnp.where(group_choice == here, -1, group_choice * per_group + rank)
    unseating = slot[:, None] == jnp.arange(tok_rows, dtype=jnp.int32)[None, :]
    return (dot(unseating.astype(jnp.bfloat16), home) + kept).astype(jnp.bfloat16)


def solution(mesh):
    groups = mesh.shape["ep"] // GROUP_SIZE
    split = Mesh(
        mesh.devices.reshape(mesh.shape["grp"], groups, GROUP_SIZE, mesh.shape["tp"]),
        ("grp", "g", "m", "tp"),
    )
    placed = (
        P(GRP_EP, "tp"),
        P(GRP_EP),
        P(GRP_EP, None),
        P(GRP_EP),
        P(GRP_EP, None),
        P(),
        P(EP, None, "tp"),
        P(EP, None, "tp"),
        P(EP, None, "tp"),
    )
    return jax.shard_map(
        layer, mesh=split, in_specs=placed, out_specs=P(GRP_EP, "tp"), check_vma=False
    )
```

```python
import functools

import jax
import jax.numpy as jnp
from jax import lax
from jax.experimental import pallas as pl
from jax.experimental.pallas import tpu as pltpu
from jax.sharding import Mesh
from jax.sharding import PartitionSpec as P


GROUP_SIZE = 8
TILE = 8
LANES = 128
EP = ("g", "m")
GRP_EP = ("grp", "g", "m")
BLOCK = ("tp", "m")


def exchange(array, axis):
    return lax.all_to_all(array, axis, 0, 0, tiled=True)


def shifted(array, axis, by):
    length = lax.axis_size(axis)
    return lax.ppermute(array, axis, [(a, (a + by) % length) for a in range(length)])


def up_to(length, tile):
    return -(-length // tile) * tile


def around(array, axis):
    one = shifted(array, axis, 3)
    three = shifted(array, axis, 1)
    half = array.shape[0] // 2
    top = shifted(one[:half], axis, 3)
    bottom = shifted(three[half:], axis, 1)
    return [one, three], [top, bottom]


def dot(a, b):
    return jnp.dot(a, b, preferred_element_type=jnp.float32)


def fetch(sources, slots, semaphores):
    copies = [
        pltpu.make_async_copy(source, slot, semaphores.at[i])
        for i, (source, slot) in enumerate(zip(sources, slots, strict=True))
    ]
    for copy in copies:
        copy.start()
    return copies


def gated(both, units):
    gate, up = both[:, :units], both[:, units:]
    return (gate / (1.0 + jnp.exp(-gate)) * up).astype(jnp.bfloat16)


def iota(shape, dim):
    return lax.broadcasted_iota(jnp.int32, shape, dim)


def ones(condition):
    return jnp.where(condition, 1.0, 0.0).astype(jnp.bfloat16)


def join(gate, up, joined, held, semaphores):
    chunks = semaphores.shape[1]
    units, count = gate.shape[1], gate.shape[0] // chunks
    arriving = []
    for c in range(chunks):
        rows = pl.ds(c * count, count)
        for i, side in enumerate((gate, up)):
            slot = held.at[rows, pl.ds(i * units, units)]
            copy = pltpu.make_async_copy(side.at[rows, :], slot, semaphores.at[i, c])
            copy.start()
            arriving.append(copy)
    leaving = []
    for c in range(chunks):
        rows = pl.ds(c * count, count)
        arriving[2 * c].wait()
        arriving[2 * c + 1].wait()
        copy = pltpu.make_async_copy(held.at[rows, :], joined.at[rows, :], semaphores.at[2, c])
        copy.start()
        leaving.append(copy)
    for copy in leaving:
        copy.wait()


def depart(group, choice, group_share, expert_share, tokens, blocks, ranks):
    groups, _, lanes = blocks.shape
    count, width = tokens.shape
    chunks, per_group = width // lanes, count // groups
    group = group[...].reshape(1, count)
    member = group == iota((groups, count), 0)
    earlier = dot(ones(member), ones(iota((count, count), 0) < iota((count, count), 1)))
    rank = jnp.sum(jnp.where(member, earlier, 0.0), 0, keepdims=True).astype(jnp.int32)
    ranks[...] = rank
    seating = ones(iota((count, count), 0) == group * per_group + rank)
    seated = dot(seating, tokens[...]).astype(jnp.bfloat16)
    mixing = group_share[...].reshape(1, count) * expert_share[...]
    mixing = mixing / jnp.sum(expert_share[...], 0, keepdims=True)
    coarse = mixing.astype(jnp.bfloat16).astype(jnp.float32)
    fine = mixing - coarse
    choice = choice[...].astype(jnp.float32)
    facts = jnp.zeros((TILE, count), jnp.float32)
    for i, pair in enumerate((choice, coarse, fine)):
        for k in range(2):
            facts = jnp.where(iota((TILE, count), 0) == 2 * i + k, pair[k : k + 1], facts)
    spoken = [jnp.where(group == g, facts, 0.0) for g in range(groups)]
    spoken = jnp.concatenate(spoken, 0).astype(jnp.bfloat16)
    columns = ones(iota((lanes, count), 0) == rank)
    told = lax.dot_general(
        spoken, columns, (((1,), (1,)), ((), ())), preferred_element_type=jnp.float32
    ).astype(jnp.bfloat16)
    for g in range(groups):
        for c in range(chunks):
            piece = seated[g * per_group : (g + 1) * per_group, c * lanes : (c + 1) * lanes]
            blocks[g, c * per_group : (c + 1) * per_group, :] = piece
        blocks[g, chunks * per_group :, :] = told[g * TILE : (g + 1) * TILE]


def arrive(capacity, landed, buffer, places, shares, seats):
    groups, lines, lanes = landed.shape
    parts, count, width = buffer.shape
    chunks = width // lanes
    per_group = (lines - TILE) // chunks
    members = GROUP_SIZE
    depth = count // members
    sources = groups // parts
    told = landed[:, chunks * per_group :, :].astype(jnp.float32)
    told = told.reshape(groups * TILE, lanes).astype(jnp.bfloat16)
    wanted = (6 * groups, groups * TILE)
    row = iota(wanted, 0)
    pick = iota(wanted, 1) == lax.rem(row, groups) * TILE + lax.div(row, groups)
    heard = dot(ones(pick), told)
    facts = [heard[i * groups : (i + 1) * groups] for i in range(6)]
    choices = [fact.astype(jnp.int32) for fact in facts[:2]]
    inside = iota((groups, lanes), 1) < per_group
    named = []
    for e in range(members):
        hit = (choices[0] == e) | (choices[1] == e)
        named.append(jnp.where(hit & inside, 1.0, 0.0))
    named = jnp.concatenate(named, 0).astype(jnp.bfloat16)
    earlier = dot(named, ones(iota((lanes, lanes), 0) < iota((lanes, lanes), 1)))
    source = iota((groups, lanes), 0)
    local = []
    for k in range(2):
        seat = jnp.zeros((groups, lanes), jnp.float32)
        for e in range(members):
            seat = jnp.where(choices[k] == e, earlier[e * groups : (e + 1) * groups], seat)
        place = choices[k] * depth + lax.rem(source, sources) * capacity + seat.astype(jnp.int32)
        local.append(jnp.where(inside, place, -1))
        places[k] = jnp.where(inside, lax.div(source, sources) * count + place, -1)
        shares[k] = facts[2 + k] + facts[4 + k]
    for g in range(groups):
        seats[g, per_group:, :] = jnp.zeros((lanes - per_group, width), jnp.bfloat16)
        for c in range(chunks):
            piece = landed[g, c * per_group : (c + 1) * per_group, :]
            seats[g, :per_group, c * lanes : (c + 1) * lanes] = piece
    rows = iota((count, lanes), 0)
    for p in range(parts):
        spread = []
        for g in range(p * sources, (p + 1) * sources):
            hit = (rows == local[0][g : g + 1]) | (rows == local[1][g : g + 1])
            spread.append(ones(hit))
        spread = jnp.concatenate(spread, 1)
        held = seats[p * sources : (p + 1) * sources].reshape(sources * lanes, width)
        buffer[p] = dot(spread, held).astype(jnp.bfloat16)


def gated(gate, up):
    return (gate / (1.0 + jnp.exp(-gate)) * up).astype(jnp.bfloat16)


def place(hidden, me, offset, parts, piece):
    units = piece.shape[1]
    at = pl.multiple_of(lax.rem(me[0] + offset, parts) * units, units)
    hidden[:, pl.ds(at, units)] = piece


def by_halves(whole, top, bottom):
    half = top.shape[0]
    return dot(whole[:, :half], top[...]) + dot(whole[:, half:], bottom[...])


def main_part(me, gains, *refs):
    given, (hidden_out, results), (rows, *slots) = refs[:10], refs[10:12], refs[12:22]
    normed, hidden, pieces, semaphores, leaving = refs[22:]
    gate, up, one, three, top, bottom, *down = slots
    arrived, *copies = fetch(given, (rows, *slots), semaphores)
    parts, _, width = rows.shape
    units = gate.shape[1]
    total = None
    arrived.wait()
    for t in range(parts):
        values = rows[t].astype(jnp.float32)
        squares = jnp.sum(values * values, -1, keepdims=True)
        total = squares if total is None else total + squares
    inv_rms = lax.rsqrt(total / (parts * width) + 1e-06)
    for t in range(parts):
        scaled = rows[t].astype(jnp.float32) * inv_rms * gains[t][None, :]
        normed[:, t * width : (t + 1) * width] = scaled.astype(jnp.bfloat16)
    copies[0].wait()
    copies[1].wait()
    piece = gated(dot(normed[...], gate[...]), dot(normed[...], up[...]))
    place(hidden, me, 0, parts, piece)
    for copy, slot, offset in zip(copies[2:4], (one, three), (1, 3), strict=True):
        copy.wait()
        both = dot(normed[...], slot[...])
        place(hidden, me, offset, parts, gated(both[:, :units], both[:, units:]))
    copies[4].wait()
    copies[5].wait()
    both = by_halves(normed, top, bottom)
    place(hidden, me, 2, parts, gated(both[:, :units], both[:, units:]))
    out = [pltpu.make_async_copy(hidden, hidden_out, leaving.at[3])]
    out[0].start()
    for i, offset in enumerate((0, 1, 3)):
        copies[6 + i].wait()
        pieces[i] = dot(hidden[...], down[i][...]).astype(pieces.dtype)
        owner = lax.rem(me[0] + offset, parts)
        out.append(pltpu.make_async_copy(pieces.at[i], results.at[owner], leaving.at[i]))
        out[-1].start()
    for copy in out:
        copy.wait()


def last_part(me, *refs):
    given, results, slots, piece, semaphores = refs[:3], refs[4], refs[5:8], refs[8], refs[9]
    for copy in fetch(given, slots, semaphores):
        copy.wait()
    hidden, top, bottom = slots
    piece[...] = by_halves(hidden, top, bottom).astype(piece.dtype)
    owner = lax.rem(me[0] + 2, results.shape[0])
    copy = pltpu.make_async_copy(piece, results.at[owner], semaphores.at[3])
    copy.start()
    copy.wait()


VMEM = pl.BlockSpec(memory_space=pltpu.VMEM)
HBM = pl.BlockSpec(memory_space=pltpu.HBM)
SMEM = pl.BlockSpec(memory_space=pltpu.SMEM)


def shaped(shape, dtype=jnp.bfloat16):
    return jax.ShapeDtypeStruct(shape, dtype)


def slots_for(arrays):
    return [pltpu.VMEM(a.shape, a.dtype) for a in arrays]


def expert(rows, norm_gain, gate, up, down, gate_up_ring, down_ring, me):
    parts, count, width = rows.shape
    units = gate.shape[1]
    me = me.reshape(1)
    near, far = gate_up_ring
    near_down, far_down = down_ring
    given = [rows, gate, up, *near, *far, down, *near_down]
    whole = shaped((count, parts * units))
    hidden, results = pl.pallas_call(
        main_part,
        out_shape=(whole, shaped((parts, count, width))),
        in_specs=[SMEM, VMEM] + [HBM] * len(given),
        out_specs=(HBM, HBM),
        scratch_shapes=slots_for(given)
        + slots_for([shaped((count, parts * width)), whole, shaped((3, count, width))])
        + [pltpu.SemaphoreType.DMA((len(given),)), pltpu.SemaphoreType.DMA((4,))],
        name="main_part",
    )(me, norm_gain.reshape(parts, width), *given)
    given = [hidden, *far_down]
    return pl.pallas_call(
        last_part,
        out_shape=shaped((parts, count, width)),
        in_specs=[SMEM] + [HBM] * 4,
        out_specs=HBM,
        input_output_aliases={4: 0},
        scratch_shapes=slots_for(given)
        + slots_for([shaped((count, width))])
        + [pltpu.SemaphoreType.DMA((4,))],
        name="last_part",
    )(me, *given, results)


def layer(
    tokens,
    group_choice,
    expert_choice,
    group_weight,
    expert_weight,
    norm_gain,
    w_gate,
    w_up,
    w_down,
):
    tok_rows, piece_width = tokens.shape
    groups = lax.axis_size("g")
    members = lax.axis_size("m")
    tp_count = lax.axis_size("tp")
    me = lax.axis_index("tp")
    per_group = tok_rows // groups
    mean_load = 2 * tok_rows // (groups * members)
    capacity = mean_load + min(mean_load // 2, per_group - mean_load)
    chunks = piece_width // LANES
    depth = up_to(groups // tp_count * capacity, TILE)

    both = shaped((w_gate.shape[1], 2 * w_gate.shape[2]))
    joined = pl.pallas_call(
        join,
        out_shape=both,
        in_specs=[HBM, HBM],
        out_specs=HBM,
        scratch_shapes=slots_for([both]) + [pltpu.SemaphoreType.DMA((3, 4))],
        name="join",
    )(w_gate[0], w_up[0])
    gate_up_ring = around(joined, "tp")
    down_ring = around(w_down[0], "tp")

    blocks, rank = pl.pallas_call(
        depart,
        out_shape=(
            shaped((groups, chunks * per_group + TILE, LANES)),
            shaped((1, tok_rows), jnp.int32),
        ),
        in_specs=[VMEM] * 5,
        out_specs=(VMEM, VMEM),
        name="depart",
    )(group_choice, expert_choice.T, group_weight, expert_weight.T, tokens)
    rank = rank[0]
    landed = exchange(blocks, "g")

    facts_shape = (2, groups, LANES)
    buffer, targets, shares = pl.pallas_call(
        functools.partial(arrive, capacity),
        out_shape=(
            shaped((tp_count, members * depth, piece_width)),
            shaped(facts_shape, jnp.int32),
            shaped(facts_shape, jnp.float32),
        ),
        in_specs=[VMEM],
        out_specs=(VMEM, VMEM, VMEM),
        scratch_shapes=[pltpu.VMEM((groups, LANES, piece_width), jnp.bfloat16)],
        name="arrive",
    )(landed)
    rows = exchange(buffer.reshape(tp_count * members, depth, piece_width), BLOCK)
    rows = rows.reshape(tp_count, members * depth, piece_width)
    results = expert(
        rows, norm_gain, w_gate[0], w_up[0], w_down[0], gate_up_ring, down_ring, me
    )

    places = jnp.arange(tp_count * members * depth, dtype=jnp.int32)
    targets, shares, results = lax.optimization_barrier((targets, shares, results))
    coarse = lax.reduce_precision(shares, 8, 7)
    mixers = []
    for share in (coarse, shares - coarse):
        weights = 0.0
        for k in range(2):
            back = targets[k][:, :per_group].reshape(-1)
            part = share[k][:, :per_group].reshape(-1)
            weights += jnp.where(back[:, None] == places[None, :], part[:, None], 0.0)
        mixers.append(weights.astype(jnp.bfloat16))
    mixers = lax.optimization_barrier(mixers)
    returned = exchange(results.reshape(tp_count * members, depth, piece_width), BLOCK)
    returned = returned.reshape(-1, piece_width)
    combined = sum(dot(weights, returned) for weights in mixers).astype(jnp.bfloat16)
    home = exchange(combined.reshape(groups, per_group, piece_width), "g")
    home = home.reshape(tok_rows, piece_width)
    here = lax.axis_index("g")
    seats = jnp.arange(per_group, dtype=jnp.int32)[None, :]
    stayed = (group_choice == here)[:, None] & (rank[:, None] == seats)
    own = lax.dynamic_slice_in_dim(combined, here * per_group, per_group, 0)
    kept = lax.optimization_barrier(dot(stayed.astype(jnp.bfloat16), own))
    slot = jnp.where(group_choice == here, -1, group_choice * per_group + rank)
    unseating = slot[:, None] == jnp.arange(tok_rows, dtype=jnp.int32)[None, :]
    return (dot(unseating.astype(jnp.bfloat16), home) + kept).astype(jnp.bfloat16)


def solution(mesh):
    groups = mesh.shape["ep"] // GROUP_SIZE
    split = Mesh(
        mesh.devices.reshape(mesh.shape["grp"], groups, GROUP_SIZE, mesh.shape["tp"]),
        ("grp", "g", "m", "tp"),
    )
    placed = (
        P(GRP_EP, "tp"),
        P(GRP_EP),
        P(GRP_EP, None),
        P(GRP_EP),
        P(GRP_EP, None),
        P(),
        P(EP, None, "tp"),
        P(EP, None, "tp"),
        P(EP, None, "tp"),
    )
    return jax.shard_map(
        layer, mesh=split, in_specs=placed, out_specs=P(GRP_EP, "tp"), check_vma=False
    )
```
